32 devices in a mesh: sp: 8 (over z, y), tp: 4 (over x, core).
Axes of the slice: x: 2, y: 2, z: 4, core: 2. Of those that a mesh axis runs over, the one named last changes fastest.
Arguments:
- moe_input: bfloat16 [2048, 2048], P('sp'), may hold values from -17.5 to 17.5
- cotangent: bfloat16 [2048, 2048], P('sp'), may hold values from -6 to 6
- routes: int32 [2048, 2], P('sp'), may hold values from 0 to 7, all different within a row; in each aligned block of 256 rows (0 to 255, 256 to 511, ...) at most 80 rows name the same one
- route_weights: float32 [2048, 2], P('sp'), may hold values from 0.2 to 1
- gate_weight: bfloat16 [8, 2048, 2048], P('sp', None, 'tp'), may hold values from -0.125 to 0.125
- up_weight: bfloat16 [8, 2048, 2048], P('sp', None, 'tp'), may hold values from -0.125 to 0.125
- down_weight: bfloat16 [8, 2048, 2048], P('sp', 'tp'), may hold values from -0.125 to 0.125
- out_weight: bfloat16 [2048, 2048], P(None, 'tp'), may hold values from -0.125 to 0.125
- mixer_output: bfloat16 [2048, 2048], P('sp', 'tp'), may hold values from -6 to 6
- queries: bfloat16 [2048, 2048], P('sp', 'tp'), may hold values from -6 to 6
- key_vectors: bfloat16 [2048, 2048], P('sp', 'tp'), may hold values from -0.75 to 0.75
- value_vectors: bfloat16 [2048, 2048], P('sp', 'tp'), may hold values from -6 to 6
- log_decay: float32 [2048, 32], P('sp', 'tp'), may hold values from -0.85 to 0
- block_states: bfloat16 [16, 32, 64, 64], P('sp', 'tp'), may hold values from -1.5 to 1.5
Outputs:
- grad_gate: float32 [8, 2048, 2048], P('sp', None, 'tp')
- grad_up: float32 [8, 2048, 2048], P('sp', None, 'tp')
- grad_down: float32 [8, 2048, 2048], P('sp', 'tp')
- grad_out: float32 [2048, 2048], P('sp', 'tp')
- grad_queries: bfloat16 [2048, 2048], P('sp', 'tp')
- grad_keys: bfloat16 [2048, 2048], P('sp', 'tp')
- grad_values: bfloat16 [2048, 2048], P('sp', 'tp')
The draws below stay inside these ranges and needn't reach their ends.
Inputs may be any that keep to these rules, and one draw needn't show every extreme that they name: `routes`: each row names 2 different experts. Among the rows of one device no expert is named by more than 80 rows, and in every draw some device's rows name some expert exactly 80 times.
All inputs are finite; a program needn't handle non-finite values.
Results may differ from the reference program's by a relative error of at most 0.02.
Values may be sent and summed in bfloat16 or wider, within the bound.
A program may use at most 128 MiB of HBM per device.

```python
import math
import jax
import jax.numpy as jnp
import numpy as np
from jax import lax

D = 2048
FF = 2048
HEADS = 32
HEAD_DIM = 64
EXPERTS = 8
TOP_K = 2
TOK_DEV = 256
TOKENS = 2048
CAP = 80
BLK = 128
NBLK = 16
N_SP = 8
N_TP = 4


def draw_moe_input(key, part):
    key_rows, key_values = jax.random.split(key)
    row_scale = jnp.exp(jax.random.uniform(key_rows, (TOKENS, 1), jnp.float32, jnp.log(0.25), jnp.log(3.0)))
    values = jnp.clip(jax.random.normal(key_values, (TOKENS, D), jnp.float32), -3.5, 3.5)
    return (values * row_scale).astype(jnp.bfloat16)


def draw_log_decay(key, part):
    subkeys = jax.random.split(key, 9)
    fast_edge = 0.3
    middle_edge = 0.55
    head_class = jax.random.uniform(subkeys[0], (HEADS,), jnp.float32)
    fast_rate = jax.random.uniform(subkeys[1], (HEADS,), jnp.float32, 1.0 / 50.0, 1.0 / 30.0)
    middle_rate = jnp.exp(jax.random.uniform(subkeys[8], (HEADS,), jnp.float32, jnp.log(1.0 / 2048.0), jnp.log(1.0 / 256.0)))
    chain_rate = jax.random.uniform(subkeys[2], (HEADS,), jnp.float32, 0.05, 0.15) / TOKENS
    base_rate = jnp.where(head_class < fast_edge, fast_rate, jnp.where(head_class < middle_edge, middle_rate, chain_rate))
    segment_factor = jax.random.uniform(subkeys[3], (TOKENS // TOK_DEV, 1, HEADS), jnp.float32, 1.0, 3.0)
    jitter = jax.random.uniform(subkeys[4], (TOKENS // TOK_DEV, TOK_DEV, HEADS), jnp.float32, 0.5, 1.5)
    forgetting_factor_matrix = (segment_factor * jitter).reshape(TOKENS, HEADS) * base_rate[None, :]
    primary_expert_index = jax.random.randint(subkeys[5], (HEADS,), 0, TOKENS)
    runner_expert_index = (primary_expert_index + 1 + jax.random.randint(subkeys[6], (HEADS,), 0, TOKENS - 1)) % TOKENS
    discarded_log_terms = jnp.log(jax.random.uniform(subkeys[7], (2, HEADS), jnp.float32, 0.5, 0.8))
    sequence_indices = jnp.arange(TOKENS, dtype=jnp.int32)[:, None]
    exchange_batches = jnp.where(sequence_indices == primary_expert_index[None, :], discarded_log_terms[0][None, :], 0.0)
    exchange_batches = exchange_batches + jnp.where(sequence_indices == runner_expert_index[None, :], discarded_log_terms[1][None, :], 0.0)
    return (exchange_batches - forgetting_factor_matrix).astype(jnp.float32)


def spiked(values, own_key, source, target, shards_of, factor):
    owner, partner = [(jnp.arange(values.shape[axis_at]) // (values.shape[axis_at] // shards_of)).reshape([-1 if axis == axis_at else 1 for axis in range(values.ndim)]) for axis_at in (source, target)]
    chosen = jax.random.permutation(own_key, shards_of)[partner]
    strong = (owner == chosen) | (owner == (partner + shards_of // 2) % shards_of)
    return jnp.where(strong, factor * values, values)


def level_of(rng, shape, cuts, low, top_value):
    loudness, own = 1.0, jax.random.fold_in(rng, 6)
    for position, shards_of in cuts:
        heights = jnp.exp(jax.random.uniform(jax.random.fold_in(own, position), (shards_of,), jnp.float32, low / len(cuts), top_value / len(cuts)))
        loudness = loudness * jnp.repeat(heights, shape[position] // shards_of).reshape([-1 if axis == position else 1 for axis in range(len(shape))])
    return loudness


def deal_out(own_key, own, number, rows, count, top, reach, slope):
    sequence = jax.random.permutation(own_key, count)
    packed, usual = shares(count, rows * top, reach, slope, True), shares(count, rows * top, reach, slope, False)
    places = jnp.arange(count)

    def named(lengths, offset_by):
        used = int((lengths > 0).sum())
        fixed = max(1, used // 4)
        passed = fixed + (places - fixed + offset_by * (used - fixed)) % max(1, count - fixed)
        return jnp.zeros((count,), jnp.int32).at[sequence[jnp.where(places < fixed, places, passed)]].set(jnp.asarray(lengths, jnp.int32))

    lengths = jnp.where(number % 4 == 0, named(packed, number // 4), named(usual, number - number // 4 - 1))
    mixed = jax.random.permutation(jax.random.fold_in(own, 3), count)
    donor, receiver = mixed[0:count // 2 * 2:2], mixed[1:count // 2 * 2:2]
    room = jnp.minimum(lengths[donor] - 1, reach - lengths[receiver]) // 2
    room = jnp.where((donor == sequence[0]) | (receiver == sequence[0]) | (lengths[receiver] == 0), 0, jnp.maximum(room, 0))
    passed = jax.random.randint(jax.random.fold_in(own, 4), (count // 2,), 0, 1 << 20) % (room + 1)
    lengths = lengths.at[donor].add(-passed).at[receiver].add(passed)
    members = jnp.searchsorted(jnp.cumsum(lengths), jnp.arange(rows * top), side="right").astype(jnp.int32)
    table = members.reshape(top, rows).T
    table = table[jax.random.permutation(jax.random.fold_in(own, 1), rows)]
    offset_by = jax.random.randint(jax.random.fold_in(own, 2), (rows, 1), 0, top)
    return jnp.take_along_axis(table, (jnp.arange(top)[None, :] + offset_by) % top, axis=1)


def shares(number_of, total, most, skew, full):
    portions = [(1 << 20) // math.isqrt(grade ** skew) + 1 for grade in range(1, number_of + 1)]
    largest = most if full else min(most, max(-(-total // number_of), total * portions[0] // sum(portions)))
    least = 1 if total - largest >= number_of - 1 else 0
    counts, rest = [largest] + [least] * (number_of - 1), total - largest - least * (number_of - 1)
    while rest > 0:
        free = [i for i in range(1, number_of) if counts[i] < largest] or [i for i in range(1, number_of) if counts[i] < most]
        mass, budget = sum([portions[i] for i in free]), rest
        for i in free:
            extra = min(most - counts[i], max(1, budget * portions[i] // mass), rest)
            counts[i] = counts[i] + extra
            rest = rest - extra
    return np.array(counts)


def gaussian(stream_key, shape, spread, limit, cuts=(), kind=jnp.bfloat16):
    entries = spread * jax.random.normal(stream_key, shape, jnp.float32)
    if cuts:
        entries = entries * level_of(stream_key, shape, cuts, -0.22, 0.18)
    return jnp.clip(entries, -limit, limit).astype(kind)


def noise_with(key, extent, spread, bound, cuts, heavy, held_as=jnp.bfloat16):
    values = spread * jax.random.normal(key, extent, jnp.float32)
    if cuts:
        values = values * level_of(key, extent, cuts, -0.22, 0.18)
    return jnp.clip(spiked(values, jax.random.fold_in(key, 3), *heavy), -bound, bound).astype(held_as)


def setup_inputs(seed: int = 0) -> dict:
    arg_keys = jax.random.split(jax.random.key(seed), 15)
    moe_input = draw_moe_input(jax.random.fold_in(arg_keys[14], 71), 0)
    cotangent = noise_with(arg_keys[1], (TOKENS, D), 1.0, 6.0, ((0, 8),), (0, 1, 8, 2.0))
    routes_keys = jax.random.split(jax.random.fold_in(arg_keys[2], 1), TOKENS // TOK_DEV)
    routes_turns = jax.random.permutation(jax.random.fold_in(arg_keys[2], 3), TOKENS // TOK_DEV)
    routes = jax.vmap(lambda own, number: deal_out(jax.random.fold_in(arg_keys[2], 2), own, number, TOK_DEV, EXPERTS, TOP_K, CAP, 1))(routes_keys, routes_turns).reshape((TOKENS, TOP_K))
    route_weights = jnp.clip(0.2 + 0.8 * jax.random.uniform(arg_keys[3], (TOKENS, TOP_K), jnp.float32) ** level_of(arg_keys[3], (TOKENS, TOP_K), ((0, 8),), -0.2, 0.2), 0.2, 1.0)
    gate_weight = gaussian(arg_keys[4], (EXPERTS, D, FF), D ** -0.5, 0.125, ((0, 8), (2, 4)))
    up_weight = gaussian(arg_keys[5], (EXPERTS, D, FF), D ** -0.5, 0.125, ((0, 8), (2, 4)))
    down_weight = gaussian(arg_keys[6], (EXPERTS, FF, D), FF ** -0.5, 0.125, ((0, 8), (1, 4)))
    out_weight = gaussian(arg_keys[7], (D, HEADS * HEAD_DIM), D ** -0.5, 0.125, ((1, 4),))
    mixer_output = gaussian(arg_keys[8], (TOKENS, HEADS * HEAD_DIM), 1.0, 6.0, ((0, 8), (1, 4)))
    queries = gaussian(arg_keys[9], (TOKENS, HEADS * HEAD_DIM), 1.0, 6.0, ((0, 8), (1, 4)))
    key_vectors = gaussian(arg_keys[10], (TOKENS, HEADS * HEAD_DIM), HEAD_DIM ** -0.5, 0.75, ((0, 8), (1, 4)))
    value_vectors = gaussian(arg_keys[11], (TOKENS, HEADS * HEAD_DIM), 1.0, 6.0, ((0, 8), (1, 4)))
    log_decay = draw_log_decay(jax.random.fold_in(arg_keys[14], 71), 0)
    block_states = gaussian(arg_keys[13], (NBLK, HEADS, HEAD_DIM, HEAD_DIM), 0.25, 1.5, ((0, 8), (1, 4)))
    return {"moe_input": moe_input, "cotangent": cotangent, "routes": routes, "route_weights": route_weights, "gate_weight": gate_weight, "up_weight": up_weight, "down_weight": down_weight, "out_weight": out_weight, "mixer_output": mixer_output, "queries": queries, "key_vectors": key_vectors, "value_vectors": value_vectors, "log_decay": log_decay, "block_states": block_states}


clamp_limit = 7.0
sigmoid_sharpness = 1.702


def round_keep(values):
    return lax.optimization_barrier(values.astype(jnp.bfloat16)).astype(jnp.float32)


def pair_slots(routes_blocks):
    flat_routes = routes_blocks.reshape(routes_blocks.shape[0], -1)
    onehot = (flat_routes[:, :, None] == jnp.arange(EXPERTS, dtype=jnp.int32)[None, None, :]).astype(jnp.int32)
    before = jnp.cumsum(onehot, axis=1) - onehot
    return (flat_routes * CAP + jnp.sum(before * onehot, axis=2)).astype(jnp.int32)


def expert_grads(expert_rows, expert_cotangent, w_gate, w_up, w_down):
    gate_pre = jnp.dot(expert_rows, w_gate, preferred_element_type=jnp.float32)
    up_pre = jnp.dot(expert_rows, w_up, preferred_element_type=jnp.float32)
    act_grad = jnp.dot(expert_cotangent, w_down.T, preferred_element_type=jnp.float32)
    clamped = jnp.minimum(gate_pre, clamp_limit)
    logistic = jax.nn.sigmoid(sigmoid_sharpness * clamped)
    linear = jnp.clip(up_pre, -clamp_limit, clamp_limit)
    activation = (clamped * logistic * (linear + 1.0)).astype(jnp.bfloat16)
    slope_term = logistic + sigmoid_sharpness * clamped * logistic * (1.0 - logistic)
    gate_grad = jnp.where(gate_pre < clamp_limit, act_grad * (linear + 1.0) * slope_term, 0.0).astype(jnp.bfloat16)
    up_grad = jnp.where(jnp.abs(up_pre) < clamp_limit, act_grad * clamped * logistic, 0.0).astype(jnp.bfloat16)
    group_width = w_gate.shape[1] // N_TP
    gate_split = gate_grad.astype(jnp.float32).reshape(-1, N_TP, group_width)
    up_split = up_grad.astype(jnp.float32).reshape(-1, N_TP, group_width)
    partials = jnp.einsum("rgf,dgf->grd", gate_split, w_gate.astype(jnp.float32).reshape(-1, N_TP, group_width))
    partials = partials + jnp.einsum("rgf,dgf->grd", up_split, w_up.astype(jnp.float32).reshape(-1, N_TP, group_width))
    pair_grad = jnp.sum(round_keep(partials), axis=0).astype(jnp.bfloat16)
    grad_gate = jnp.dot(expert_rows.T, gate_grad, preferred_element_type=jnp.float32)
    grad_up = jnp.dot(expert_rows.T, up_grad, preferred_element_type=jnp.float32)
    grad_down = jnp.dot(activation.T, expert_cotangent, preferred_element_type=jnp.float32)
    return pair_grad, grad_gate, grad_up, grad_down


def retention_grads(queries, key_vectors, value_vectors, grad_mix, log_decay, block_states):
    blocks = TOKENS // BLK
    block_shape = (blocks, BLK, HEADS, HEAD_DIM)
    query_blocks = queries.astype(jnp.float32).reshape(block_shape)
    key_blocks = key_vectors.astype(jnp.float32).reshape(block_shape)
    value_blocks = value_vectors.astype(jnp.float32).reshape(block_shape)
    grad_blocks = grad_mix.astype(jnp.float32).reshape(block_shape)
    states = block_states.astype(jnp.float32)
    cumulative = jnp.cumsum(log_decay.reshape(blocks, BLK, HEADS), axis=1)
    block_ends = cumulative[:, -1, :]
    to_end = jnp.exp(block_ends[:, None, :] - cumulative)
    from_start = jnp.exp(cumulative)
    per_attention_head = jnp.transpose(cumulative, (0, 2, 1))
    differences = per_attention_head[:, :, :, None] - per_attention_head[:, :, None, :]
    causal = jnp.arange(BLK, dtype=jnp.int32)[:, None] >= jnp.arange(BLK, dtype=jnp.int32)[None, :]
    decays = jnp.where(causal, jnp.exp(jnp.minimum(differences, 0.0)), 0.0)
    weighted_grad = round_keep(jnp.einsum("nthe,nshe->nhts", grad_blocks, value_blocks) * decays)
    weighted_score = round_keep(jnp.einsum("nthd,nshd->nhts", query_blocks, key_blocks) * decays)
    query_intra = jnp.einsum("nhts,nshd->nthd", weighted_grad, key_blocks)
    query_carry = jnp.einsum("nthe,nhde->nthd", grad_blocks, states) * from_start[..., None]
    grad_queries = (query_intra + query_carry).astype(jnp.bfloat16).reshape(TOKENS, HEADS * HEAD_DIM)
    scaled_queries = round_keep(query_blocks * from_start[..., None])
    outer_terms = jnp.einsum("nthd,nthe->nhde", scaled_queries, grad_blocks)
    end_factor = jnp.exp(block_ends)

    def suffix_step(state_grad, inputs):
        factor, outer_block = inputs
        return factor[:, None, None] * state_grad + outer_block, state_grad

    start_grad = jnp.zeros((HEADS, HEAD_DIM, HEAD_DIM), jnp.float32)
    _, leaving = lax.scan(suffix_step, start_grad, (end_factor, outer_terms), reverse=True)
    carried = round_keep(leaving)
    key_intra = jnp.einsum("nhts,nthd->nshd", weighted_grad, query_blocks)
    value_intra = jnp.einsum("nhts,nthe->nshe", weighted_score, grad_blocks)
    key_carry = jnp.einsum("nshe,nhde->nshd", value_blocks, carried) * to_end[..., None]
    value_carry = jnp.einsum("nshd,nhde->nshe", key_blocks, carried) * to_end[..., None]
    grad_keys = (key_intra + key_carry).astype(jnp.bfloat16).reshape(TOKENS, HEADS * HEAD_DIM)
    grad_values = (value_intra + value_carry).astype(jnp.bfloat16).reshape(TOKENS, HEADS * HEAD_DIM)
    return grad_queries, grad_keys, grad_values


def reference(moe_input, cotangent, routes, route_weights, gate_weight, up_weight, down_weight, out_weight, mixer_output, queries, key_vectors, value_vectors, log_decay, block_states):
    pair_count = TOK_DEV * TOP_K
    slot_index = pair_slots(routes.reshape(N_SP, TOK_DEV, TOP_K))
    source = jnp.arange(N_SP, dtype=jnp.int32)[:, None]
    pair_ids = (source * pair_count + jnp.arange(pair_count, dtype=jnp.int32)[None, :]).astype(jnp.int32)
    slot_pair = jnp.full((N_SP, EXPERTS * CAP), TOKENS * TOP_K, jnp.int32).at[source, slot_index].set(pair_ids)
    tables = jnp.transpose(slot_pair.reshape(N_SP, EXPERTS, CAP), (1, 0, 2)).reshape(EXPERTS, N_SP * CAP)
    zero_row = jnp.zeros((1, D), jnp.bfloat16)
    scaled = (route_weights[:, :, None] * cotangent.astype(jnp.float32)[:, None, :]).astype(jnp.bfloat16)
    scaled = jnp.concatenate([scaled.reshape(TOKENS * TOP_K, D), zero_row], axis=0)
    inputs_padded = jnp.concatenate([moe_input, zero_row], axis=0)

    def one_expert(operands):
        table, w_gate, w_up, w_down = operands
        return expert_grads(inputs_padded[table // TOP_K], scaled[table], w_gate, w_up, w_down)

    pair_rows, grad_gate, grad_up, grad_down = lax.map(one_expert, (tables, gate_weight, up_weight, down_weight))
    pair_sum = jnp.zeros((TOKENS * TOP_K + 1, D), jnp.float32).at[tables.reshape(-1)].add(pair_rows.reshape(-1, D).astype(jnp.float32))
    token_sum = jnp.sum(pair_sum[:TOKENS * TOP_K].reshape(TOKENS, TOP_K, D), axis=1)
    residual_grad = (cotangent.astype(jnp.float32) + token_sum).astype(jnp.bfloat16)
    grad_out = jnp.dot(residual_grad.T, mixer_output, preferred_element_type=jnp.float32)
    grad_mix = jnp.dot(residual_grad, out_weight, preferred_element_type=jnp.float32).astype(jnp.bfloat16)
    grad_queries, grad_keys, grad_values = retention_grads(queries, key_vectors, value_vectors, grad_mix, log_decay, block_states)
    return (grad_gate, grad_up, grad_down, grad_out, grad_queries, grad_keys, grad_values)
```

```python
import functools

import jax
import jax.numpy as jnp
from jax import lax
from jax.experimental import pallas as pl
from jax.experimental.pallas import tpu as pltpu
from jax.sharding import PartitionSpec as P

TOP_K = 2
MESH = pl.DeviceIdType.MESH
VMEM = pl.BlockSpec(memory_space=pltpu.VMEM)
ANY = pl.BlockSpec(memory_space=pl.ANY)

clamp_limit = 7.0
sigmoid_sharpness = 1.702


def contract_rows(left, right):
    return lax.dot_general(
        left, right, (((0,), (0,)), ((), ())), preferred_element_type=jnp.float32
    )


def contract_cols(left, right):
    return lax.dot_general(
        left, right, (((1,), (1,)), ((), ())), preferred_element_type=jnp.float32
    )


def peer_order(peers):
    near = [k for k in range(1, peers) if k < peers // 2]
    far = [k for k in range(1, peers) if k >= peers // 2]
    order = []
    while near or far:
        if near:
            order.append(near.pop(0))
        if far:
            order.append(far.pop(0))
    return order


def greet(peers, sp, tp):
    barrier = pltpu.get_barrier_semaphore()
    others = [(sp ^ k, tp) for k in range(1, peers)] + [(sp, tp ^ 1), (sp, tp ^ 2)]
    for other in others:
        pl.semaphore_signal(barrier, inc=1, device_id=other, device_id_type=MESH)
    pl.semaphore_wait(barrier, len(others))


def remote(src, dst, sems, kind, at, device):
    return pltpu.make_async_remote_copy(
        src_ref=src,
        dst_ref=dst,
        send_sem=sems.at[(2 * kind,) + at],
        recv_sem=sems.at[(2 * kind + 1,) + at],
        device_id=device,
        device_id_type=MESH,
    )


def exchange_start(peers, sp, tp, arrays, source, chunk, sems, local_sems):
    order = peer_order(peers)
    owns, firsts = [], {}
    for k in order:
        for a, (src, dst) in enumerate(arrays):
            copy = remote(source(src, sp ^ k), chunk(dst, sp, tp), sems, 0, (a, k), (sp ^ k, tp))
            copy.start()
            firsts[a, k] = copy
    for a, (src, dst) in enumerate(arrays):
        copy = pltpu.make_async_copy(source(src, sp), chunk(dst, sp, tp), local_sems.at[a])
        copy.start()
        owns.append(copy)
    return order, owns, firsts


def exchange_finish(peers, sp, tp, arrays, source, chunk, sems, state):
    order, owns, firsts = state
    crossings, partners, forwards = {}, {}, {}

    def forward(k):
        for a, (_, dst) in enumerate(arrays):
            crossings[a, k].wait_recv()
            here = chunk(dst, sp ^ k, tp ^ 2)
            copy = remote(here, here, sems, 3, (a, k), (sp, tp ^ 1))
            copy.start()
            forwards[a, k] = copy

    steps = [0] + order
    for i, k in enumerate(steps):
        for a, (src, dst) in enumerate(arrays):
            there = chunk(dst, sp ^ k, tp)
            if k:
                firsts[a, k].wait_recv()
                here = there
            else:
                here = source(src, sp)
            copy = remote(here, there, sems, 1, (a, k), (sp, tp ^ 2))
            copy.start()
            crossings[a, k] = copy
            copy = remote(here, there, sems, 2, (a, k), (sp, tp ^ 1))
            copy.start()
            partners[a, k] = copy
        if i >= 1:
            forward(steps[i - 1])
    forward(steps[-1])
    for copy in owns:
        copy.wait()
    for group in (partners, forwards):
        for copy in group.values():
            copy.wait_recv()
    for group in (firsts, crossings, partners, forwards):
        for copy in group.values():
            copy.wait_send()


def issue_order(peers):
    near = list(range(1, max(peers // 2, 1)))
    far = [k for k in range(1, peers) if k not in near]
    order = near[:1]
    near = near[1:]
    while near or far:
        if near:
            order.append(near.pop(0))
        if far:
            order.append(far.pop(0))
    return [0] + order


def gather_order(peers):
    order = [0]
    bit = peers // 2
    while bit:
        order = order + [k ^ bit for k in order]
        bit //= 2
    return order


def moe_kernel(
    peers,
    parts,
    cap,
    routes_ref,
    weights_ref,
    x_ref,
    cot_ref,
    gate_hbm,
    up_hbm,
    down_hbm,
    mix_ref,
    res_ref,
    xr_out,
    gr_out,
    act_out,
    gg_out,
    ug_out,
    mix_out,
    wg,
    wu,
    wd,
    xr,
    gr,
    sx,
    sg,
    pre_g,
    pre_u,
    pre_a,
    act,
    gg,
    ug,
    part,
    rx1,
    acc,
    sb,
    rx2,
    fb,
    ret,
    comb,
    mixbuf,
    dsems,
    rsems,
    tsems,
    msems,
    lsems,
    osems,
):
    sp, tp = lax.axis_index("sp"), lax.axis_index("tp")
    tokens, width = x_ref.shape[0], x_ref.shape[1] // parts
    total_rows = peers * cap
    steps = issue_order(peers)
    half = len(steps) // 2
    groups = [list(range(half)), list(range(half, peers))]
    f32, bf16 = jnp.float32, jnp.bfloat16

    loads = []
    for i, (src, dst) in enumerate(((gate_hbm, wg), (up_hbm, wu), (down_hbm, wd))):
        copy = pltpu.make_async_copy(src, dst, lsems.at[i])
        copy.start()
        loads.append(copy)
    greet(peers, sp, tp)

    def cols(t):
        return pl.ds(pl.multiple_of(t * width, width), width)

    def rows(j):
        return pl.ds(j * cap, cap)

    lane = lax.broadcasted_iota(jnp.int32, (1, 128), 1)
    expert = jnp.full((1, 128), -1, jnp.int32)
    for j, k in enumerate(steps):
        expert = jnp.where(lane == j, sp ^ k, expert)
    first = routes_ref[:, 0:1] == expert
    second = routes_ref[:, 1:2] == expert
    hits = jnp.where(first, 1.0, jnp.where(second, 1.0, 0.0))
    weight = jnp.where(first, weights_ref[:, 0:1], jnp.where(second, weights_ref[:, 1:2], 0.0))
    earlier = jnp.where(
        lax.broadcasted_iota(jnp.int32, (tokens, tokens), 0)
        > lax.broadcasted_iota(jnp.int32, (tokens, tokens), 1),
        1.0,
        0.0,
    ).astype(bf16)
    rank = jnp.dot(earlier, hits.astype(bf16), preferred_element_type=f32)
    place = jnp.where(hits > 0.5, rank, -1.0)
    place_t = place.T
    weight_t = weight.T

    x_share = x_ref[:, cols(tp)]
    c_share = cot_ref[:, cols(tp)]
    slot = lax.broadcasted_iota(jnp.int32, (cap, tokens), 0).astype(f32)
    firsts, crossings, partners, forwards = {}, {}, {}, {}
    arrays = ((sx, xr), (sg, gr))

    def spread(j):
        k = steps[j]
        here = place_t[j : j + 1, :] == slot
        pick = jnp.where(here, 1.0, 0.0)
        scale = jnp.sum(jnp.where(here, weight_t[j : j + 1, :], 0.0), axis=1, keepdims=True)
        pick = pick.astype(bf16)
        xs = jnp.dot(pick, x_share, preferred_element_type=f32).astype(bf16)
        gs = (jnp.dot(pick, c_share, preferred_element_type=f32) * scale).astype(bf16)
        if k == 0:
            xr[rows(j), cols(tp)] = xs
            gr[rows(j), cols(tp)] = gs
            pass_on(j)
        else:
            sx[rows(j), :] = xs
            sg[rows(j), :] = gs
            for a, (src, dst) in enumerate(arrays):
                copy = remote(
                    src.at[rows(j)], dst.at[rows(j), cols(tp)], dsems, 0, (a, j), (sp ^ k, tp)
                )
                copy.start()
                firsts[a, j] = copy

    def pass_on(j):
        for a, (_, dst) in enumerate(arrays):
            if steps[j]:
                firsts[a, j].wait_recv()
            here = dst.at[rows(j), cols(tp)]
            crossings[a, j] = remote(here, here, dsems, 1, (a, j), (sp, tp ^ 2))
            crossings[a, j].start()
            partners[a, j] = remote(here, here, dsems, 2, (a, j), (sp, tp ^ 1))
            partners[a, j].start()

    def forward(j):
        for a, (_, dst) in enumerate(arrays):
            crossings[a, j].wait_recv()
            here = dst.at[rows(j), cols(tp ^ 2)]
            forwards[a, j] = remote(here, here, dsems, 3, (a, j), (sp, tp ^ 1))
            forwards[a, j].start()

    def arrive(j):
        for a in range(2):
            partners[a, j].wait_recv()
            forwards[a, j].wait_recv()

    outs = []

    def put(i, src, dst):
        copy = pltpu.make_async_copy(src, dst, osems.at[i])
        copy.start()
        outs.append(copy)

    def span(g):
        return pl.ds(groups[g][0] * cap, len(groups[g]) * cap)

    def expert_pre(g):
        size = len(groups[g]) * cap
        mine = pl.ds(0, size)
        base = groups[g][0] * cap
        pre_g[mine, :] = jnp.dot(xr[span(g), :], wg[...], preferred_element_type=f32)
        pre_u[mine, :] = jnp.dot(xr[span(g), :], wu[...], preferred_element_type=f32)
        pre_a[mine, :] = contract_cols(gr[span(g), :], wd[...])

        def body(i, carry):
            at = pl.ds(pl.multiple_of(i * 16, 16), 16)
            to = pl.ds(pl.multiple_of(base + i * 16, 16), 16)
            gate_pre, up_pre, act_grad = pre_g[at, :], pre_u[at, :], pre_a[at, :]
            clamped = jnp.minimum(gate_pre, clamp_limit)
            logistic = jax.nn.sigmoid(sigmoid_sharpness * clamped)
            linear = jnp.clip(up_pre, -clamp_limit, clamp_limit)
            swish = clamped * logistic
            act[to, :] = (swish * (linear + 1.0)).astype(bf16)
            slope = logistic + sigmoid_sharpness * swish * (1.0 - logistic)
            gg[to, :] = jnp.where(
                gate_pre < clamp_limit, act_grad * (linear + 1.0) * slope, 0.0
            ).astype(bf16)
            ug[to, :] = jnp.where(
                jnp.abs(up_pre) < clamp_limit, act_grad * swish, 0.0
            ).astype(bf16)
            return carry

        lax.fori_loop(0, size // 16, body, 0)

    def expert_part(g, t):
        part[span(g), cols(t)] = (
            contract_cols(gg[span(g), :], wg[cols(t), :])
            + contract_cols(ug[span(g), :], wu[cols(t), :])
        ).astype(bf16)

    backs, overs, homes = {}, {}, {}

    def back(g, which):
        t = (tp ^ 1, tp ^ 3)[which]
        expert_part(g, t)
        for j in groups[g]:
            copy = remote(
                part.at[rows(j), cols(t)], rx1.at[which, rows(j)], rsems, which, (j,), (sp, tp ^ 1)
            )
            copy.start()
            backs[which, j] = copy

    def cross(j):
        backs[1, j].wait_recv()
        sb[rows(j), :] = (
            part[rows(j), cols(tp ^ 2)].astype(f32) + rx1[1, rows(j), :].astype(f32)
        ).astype(bf16)
        overs[j] = remote(sb.at[rows(j)], rx2.at[rows(j)], rsems, 2, (j,), (sp, tp ^ 2))
        overs[j].start()

    def settle(j):
        backs[0, j].wait_recv()
        acc[rows(j), :] = part[rows(j), cols(tp)].astype(f32) + rx1[0, rows(j), :].astype(f32)

    def home(j):
        k = steps[j]
        overs[j].wait_recv()
        final = (acc[rows(j), :] + rx2[rows(j), :].astype(f32)).astype(bf16)
        if k:
            fb[rows(j), :] = final
            homes[j] = remote(fb.at[rows(j)], ret.at[rows(j)], rsems, 3, (j,), (sp ^ k, tp))
            homes[j].start()
        else:
            ret[rows(j), :] = final

    bits = []
    bit = peers // 2
    while bit:
        bits.append(bit)
        bit //= 2
    gathers = {}

    def mix_start(i):
        count = 1 << i
        if i == 0:
            src = mix_ref.at[...]
            dst = mixbuf.at[1]
        else:
            gathers[i - 1].wait_recv()
            src = mixbuf.at[pl.ds(0, count)]
            dst = mixbuf.at[pl.ds(count, count)]
        gathers[i] = pltpu.make_async_remote_copy(
            src_ref=src,
            dst_ref=dst,
            send_sem=msems.at[0, i],
            recv_sem=msems.at[1, i],
            device_id=(sp ^ bits[i], tp),
            device_id_type=MESH,
        )
        gathers[i].start()

    scope = jax.named_scope
    eager = min(half + 1, peers)
    with scope("spread"):
        for j in range(eager):
            spread(j)
    with scope("comb"):
        mixbuf[0] = mix_ref[...]
        size = peers * cap
        slot_at = lax.broadcasted_iota(jnp.int32, (128, size), 1)
        start_at = lax.broadcasted_iota(jnp.int32, (128, size), 0) * cap
        inside = (slot_at >= start_at) & (slot_at < start_at + cap)
        member = jnp.where(inside, 1.0, 0.0)
        offset = jnp.sum(
            jnp.where(inside, (slot_at - start_at).astype(f32), 0.0), axis=0, keepdims=True
        )
        comb[...] = jnp.where(
            jnp.dot(place.astype(bf16), member.astype(bf16), preferred_element_type=f32)
            == offset,
            1.0,
            0.0,
        ).astype(bf16)

    late = list(range(eager, peers))
    for j in range(1, eager):
        with scope(f"pass{j}"):
            pass_on(j)
        if late:
            spread(late.pop(0))
        with scope(f"fwd{j - 1}"):
            forward(j - 1)
    for j in late:
        spread(j)
    with scope(f"pass{eager}"):
        pass_on(eager)
    with scope("arrive0"):
        for j in groups[0]:
            arrive(j)
        for copy in loads:
            copy.wait()
    with scope("pre0"):
        expert_pre(0)
    with scope(f"fwd{eager - 1}"):
        forward(eager - 1)
    with scope("back0"):
        back(0, 1)
        back(0, 0)
    with scope("part0"):
        expert_part(0, tp ^ 2)
        expert_part(0, tp)
    with scope("cross0a"):
        for j in groups[0][: half // 2]:
            cross(j)
    for j in range(eager + 1, peers):
        with scope(f"pass{j}"):
            pass_on(j)
        with scope(f"fwd{j - 1}"):
            forward(j - 1)
    mix_start(0)
    with scope("cross0b"):
        for j in groups[0][half // 2 :]:
            cross(j)
        for j in groups[0]:
            settle(j)
    with scope(f"fwd{peers - 1}"):
        forward(peers - 1)
    with scope("arrive1"):
        for j in groups[1]:
            arrive(j)
    put(0, xr, xr_out)
    put(1, gr, gr_out)
    with scope("pre1"):
        expert_pre(1)
    put(2, act, act_out)
    put(3, gg, gg_out)
    put(4, ug, ug_out)
    with scope("home0"):
        for j in groups[0]:
            home(j)
    with scope("back1"):
        back(1, 1)
        back(1, 0)
    with scope("part1"):
        expert_part(1, tp ^ 2)
        expert_part(1, tp)
    with scope("cross1"):
        for j in groups[1]:
            cross(j)
        for j in groups[1]:
            settle(j)
    with scope("home1"):
        for j in groups[1]:
            home(j)
    with scope("mix1"):
        mix_start(1)
    with scope("total"):
        total = cot_ref[:, cols(tp)].astype(f32)
        for g in range(2):
            for j in groups[g]:
                if steps[j]:
                    homes[j].wait_recv()
            total = total + jnp.dot(
                comb[:, groups[g][0] * cap : (groups[g][-1] + 1) * cap],
                ret[span(g), :],
                preferred_element_type=f32,
            )
        res_ref[:, cols(tp)] = total.astype(bf16)
    with scope("tail"):
        mine = res_ref.at[:, cols(tp)]
        across = remote(mine, mine, tsems, 0, (), (sp, tp ^ 2))
        across.start()
        beside = remote(mine, mine, tsems, 1, (), (sp, tp ^ 1))
        beside.start()
        across.wait_recv()
        theirs = res_ref.at[:, cols(tp ^ 2)]
        onward = remote(theirs, theirs, tsems, 2, (), (sp, tp ^ 1))
        onward.start()
        beside.wait_recv()
        onward.wait_recv()
    with scope("mixend"):
        for i in range(2, len(bits)):
            mix_start(i)
        gathers[len(bits) - 1].wait_recv()
        for m, k in enumerate(gather_order(peers)):
            put(5 + m, mixbuf.at[m], mix_out.at[sp ^ k])
    for group in (firsts, crossings, partners, forwards, backs, overs, homes, gathers):
        for copy in group.values():
            copy.wait_send()
    for copy in (across, beside, onward):
        copy.wait_send()
    for copy in outs:
        copy.wait()


def moe_backward(
    routes, route_weights, moe_input, cotangent, w_gate, w_up, w_down, mixer, peers, parts, capacity
):
    cap = -(-capacity // 16) * 16
    tokens, full = moe_input.shape
    hidden = w_gate.shape[1]
    width = full // parts
    total = peers * cap
    most = (peers - peers // 2) * cap
    bits = peers.bit_length() - 1
    bf16, f32 = jnp.bfloat16, jnp.float32

    def shape(*dims, dtype=bf16):
        return jax.ShapeDtypeStruct(dims, dtype)

    def vmem(*dims, dtype=bf16):
        return pltpu.VMEM(dims, dtype)

    return pl.pallas_call(
        functools.partial(moe_kernel, peers, parts, cap),
        out_shape=(
            shape(tokens, full),
            shape(total, full),
            shape(total, full),
            shape(total, hidden),
            shape(total, hidden),
            shape(total, hidden),
            shape(peers, *mixer.shape),
        ),
        in_specs=[VMEM] * 4 + [ANY] * 3 + [VMEM],
        out_specs=(VMEM,) + (ANY,) * 6,
        scratch_shapes=[
            vmem(full, hidden),
            vmem(full, hidden),
            vmem(hidden, full),
            vmem(total, full),
            vmem(total, full),
            vmem(total, width),
            vmem(total, width),
            vmem(most, hidden, dtype=f32),
            vmem(most, hidden, dtype=f32),
            vmem(most, hidden, dtype=f32),
            vmem(total, hidden),
            vmem(total, hidden),
            vmem(total, hidden),
            vmem(total, full),
            vmem(2, total, width),
            vmem(total, width, dtype=f32),
            vmem(total, width),
            vmem(total, width),
            vmem(total, width),
            vmem(total, width),
            vmem(tokens, total),
            vmem(peers, *mixer.shape),
            pltpu.SemaphoreType.DMA((8, 2, peers)),
            pltpu.SemaphoreType.DMA((8, peers)),
            pltpu.SemaphoreType.DMA((6,)),
            pltpu.SemaphoreType.DMA((2, bits)),
            pltpu.SemaphoreType.DMA((3,)),
            pltpu.SemaphoreType.DMA((5 + peers,)),
        ],
        compiler_params=pltpu.CompilerParams(
            collective_id=0, has_side_effects=True, vmem_limit_bytes=56 * 2**20
        ),
        name="moe_backward",
    )(routes, route_weights, moe_input, cotangent, w_gate, w_up, w_down, mixer)


def final_kernel(
    peers, parts, res_ref, tot_ref, log_ref, all_res, all_tot, all_log, sems, local_sems, st_sems
):
    sp, tp = lax.axis_index("sp"), lax.axis_index("tp")
    share = res_ref.shape[1] // parts
    greet(peers, sp, tp)

    def rows(t):
        return pl.ds(pl.multiple_of(t * share, share), share)

    def source(ref, s):
        return ref.at[s, rows(tp)]

    def chunk(ref, s, t):
        return ref.at[s, rows(t)]

    small = []
    for k in peer_order(peers):
        for i, (src, dst) in enumerate(((tot_ref, all_tot), (log_ref, all_log))):
            copy = remote(src, dst.at[sp], st_sems, i, (k,), (sp ^ k, tp))
            copy.start()
            small.append(copy)
    own = []
    for i, (src, dst) in enumerate(((tot_ref, all_tot), (log_ref, all_log))):
        copy = pltpu.make_async_copy(src, dst.at[sp], local_sems.at[1 + i])
        copy.start()
        own.append(copy)
    arrays = ((res_ref, all_res),)
    state = exchange_start(peers, sp, tp, arrays, source, chunk, sems, local_sems)
    exchange_finish(peers, sp, tp, arrays, source, chunk, sems, state)
    for copy in own + small:
        copy.wait()


def final_exchange(res, tot, logs, parts):
    peers = res.shape[0]
    return pl.pallas_call(
        functools.partial(final_kernel, peers, parts),
        out_shape=(
            jax.ShapeDtypeStruct(res.shape, res.dtype),
            jax.ShapeDtypeStruct((peers,) + tot.shape, tot.dtype),
            jax.ShapeDtypeStruct((peers,) + logs.shape, logs.dtype),
        ),
        in_specs=[ANY] * 3,
        out_specs=(ANY,) * 3,
        scratch_shapes=[
            pltpu.SemaphoreType.DMA((8, 1, peers)),
            pltpu.SemaphoreType.DMA((3,)),
            pltpu.SemaphoreType.DMA((4, peers)),
        ],
        compiler_params=pltpu.CompilerParams(collective_id=2, has_side_effects=True),
        name="final_exchange",
    )(res, tot, logs)


def retention_grads(
    queries, key_vectors, value_vectors, grad_mix, log_decay, block_states, exchange
):
    tok_dev = queries.shape[0]
    heads_local = log_decay.shape[1]
    head_dim = queries.shape[1] // heads_local
    blocks = block_states.shape[0]
    block_rows = tok_dev // blocks
    block_shape = (blocks, block_rows, heads_local, head_dim)
    query_blocks = queries.reshape(block_shape)
    key_blocks = key_vectors.reshape(block_shape)
    value_blocks = value_vectors.reshape(block_shape)
    grad_blocks = grad_mix.reshape(block_shape)
    cumulative = jnp.cumsum(log_decay.reshape(blocks, block_rows, heads_local), axis=1)
    block_ends = cumulative[:, -1, :]
    to_end = jnp.exp(block_ends[:, None, :] - cumulative)
    from_start = jnp.exp(cumulative)
    per_attention_head = jnp.transpose(cumulative, (0, 2, 1))
    differences = per_attention_head[:, :, :, None] - per_attention_head[:, :, None, :]
    causal = (
        jnp.arange(block_rows, dtype=jnp.int32)[:, None]
        >= jnp.arange(block_rows, dtype=jnp.int32)[None, :]
    )
    decays = jnp.where(causal, jnp.exp(jnp.minimum(differences, 0.0)), 0.0)
    scaled_queries = (query_blocks * from_start[..., None]).astype(jnp.bfloat16)
    outer_terms = jnp.einsum(
        "nthd,nthe->nhde", scaled_queries, grad_blocks, preferred_element_type=jnp.float32
    )
    end_factor = jnp.exp(block_ends)
    ends_before = jnp.cumsum(block_ends, axis=0) - block_ends
    device_start = jnp.exp(cumulative + ends_before[:, None, :])
    total_queries = (query_blocks * device_start[..., None]).astype(jnp.bfloat16)
    local_total = jnp.einsum(
        "thd,the->hde",
        total_queries.reshape(tok_dev, heads_local, head_dim),
        grad_mix.reshape(tok_dev, heads_local, head_dim),
        preferred_element_type=jnp.float32,
    )
    all_totals, all_logs = exchange(local_total, jnp.sum(block_ends, axis=0))
    peers, place = lax.axis_size("sp"), lax.axis_index("sp")
    where = jnp.arange(peers, dtype=jnp.int32)
    between = ((where[None, :] > place) & (where[None, :] < where[:, None]))[..., None]
    reach = jnp.sum(jnp.where(between, all_logs[None], 0.0), axis=1)
    reach = jnp.where((where > place)[:, None], jnp.exp(reach), 0.0)
    suffix = jnp.sum(reach[:, :, None, None] * all_totals.astype(jnp.float32), axis=0)
    suffix = suffix.reshape(heads_local, head_dim, head_dim)
    grad_dot = jnp.einsum(
        "nthe,nshe->nhts", grad_blocks, value_blocks, preferred_element_type=jnp.float32
    )
    weighted_grad = (grad_dot * decays).astype(jnp.bfloat16)
    score_dot = jnp.einsum(
        "nthd,nshd->nhts", query_blocks, key_blocks, preferred_element_type=jnp.float32
    )
    weighted_score = (score_dot * decays).astype(jnp.bfloat16)
    query_intra = jnp.einsum(
        "nhts,nshd->nthd", weighted_grad, key_blocks, preferred_element_type=jnp.float32
    )
    query_carry = jnp.einsum(
        "nthe,nhde->nthd", grad_blocks, block_states, preferred_element_type=jnp.float32
    )
    grad_queries = (
        (query_intra + query_carry * from_start[..., None])
        .astype(jnp.bfloat16)
        .reshape(tok_dev, -1)
    )
    key_intra = jnp.einsum(
        "nhts,nthd->nshd", weighted_grad, query_blocks, preferred_element_type=jnp.float32
    )
    value_intra = jnp.einsum(
        "nhts,nthe->nshe", weighted_score, grad_blocks, preferred_element_type=jnp.float32
    )
    state_grad = suffix
    leaving = []
    for block_id in reversed(range(blocks)):
        leaving.append(state_grad)
        state_grad = end_factor[block_id][:, None, None] * state_grad + outer_terms[block_id]
    carried = jnp.stack(leaving[::-1], axis=0).astype(jnp.bfloat16)
    key_carry = jnp.einsum(
        "nshe,nhde->nshd", value_blocks, carried, preferred_element_type=jnp.float32
    )
    value_carry = jnp.einsum(
        "nshd,nhde->nshe", key_blocks, carried, preferred_element_type=jnp.float32
    )
    grad_keys = (
        (key_intra + key_carry * to_end[..., None]).astype(jnp.bfloat16).reshape(tok_dev, -1)
    )
    grad_values = (
        (value_intra + value_carry * to_end[..., None]).astype(jnp.bfloat16).reshape(tok_dev, -1)
    )
    return (grad_queries, grad_keys, grad_values)


def shards(
    moe_input,
    cotangent,
    routes,
    route_weights,
    gate_weight,
    up_weight,
    down_weight,
    out_weight,
    mixer_output,
    queries,
    key_vectors,
    value_vectors,
    log_decay,
    block_states,
):
    tok_dev, model_width = cotangent.shape
    peers, parts = lax.axis_size("sp"), lax.axis_size("tp")
    capacity = 5 * tok_dev * TOP_K // (4 * peers)
    residual_grad, arrived_inputs, arrived_grads, activation, gate_grad, up_grad, all_mixer = (
        moe_backward(
            routes,
            route_weights,
            moe_input,
            cotangent,
            gate_weight[0],
            up_weight[0],
            down_weight[0],
            mixer_output,
            peers,
            parts,
            capacity,
        )
    )
    grad_gate = contract_rows(arrived_inputs, gate_grad)
    grad_up = contract_rows(arrived_inputs, up_grad)
    grad_down = contract_rows(activation, arrived_grads)
    all_mixer = all_mixer.reshape(peers * tok_dev, -1)
    grad_mix = jnp.dot(residual_grad, out_weight, preferred_element_type=jnp.float32).astype(
        jnp.bfloat16
    )
    slices = jnp.transpose(residual_grad.reshape(tok_dev, peers, model_width // peers), (1, 0, 2))
    gathered = []

    def exchange(total, logs):
        heads, head_dim, _ = total.shape
        packed = total.astype(jnp.bfloat16).reshape(-1, 128)
        wide = jnp.broadcast_to(logs[:, None], (heads, 128))
        all_res, all_tot, all_log = final_exchange(slices, packed, wide, parts)
        gathered.append(all_res)
        return all_tot.reshape(peers, heads, -1, 128), all_log[:, :, 0]

    grad_queries, grad_keys, grad_values = retention_grads(
        queries, key_vectors, value_vectors, grad_mix, log_decay, block_states, exchange
    )
    all_res = gathered[0].reshape(peers * tok_dev, model_width // peers)
    grad_out = contract_rows(all_res, all_mixer)
    return (
        grad_gate[None],
        grad_up[None],
        grad_down[None],
        grad_out,
        grad_queries,
        grad_keys,
        grad_values,
    )


def solution(mesh):
    return jax.shard_map(
        shards,
        mesh=mesh,
        in_specs=(
            P("sp", None),
            P("sp", None),
            P("sp", None),
            P("sp", None),
            P("sp", None, "tp"),
            P("sp", None, "tp"),
            P("sp", "tp", None),
            P(None, "tp"),
            P("sp", "tp"),
            P("sp", "tp"),
            P("sp", "tp"),
            P("sp", "tp"),
            P("sp", "tp"),
            P("sp", "tp", None, None),
        ),
        out_specs=(
            P("sp", None, "tp"),
            P("sp", None, "tp"),
            P("sp", "tp", None),
            P("sp", "tp"),
            P("sp", "tp"),
            P("sp", "tp"),
            P("sp", "tp"),
        ),
        check_vma=False,
    )
```

```python
import functools
import types

import jax
import jax.numpy as jnp
from jax import lax
from jax.experimental import pallas as pl
from jax.experimental.pallas import tpu as pltpu
from jax.sharding import PartitionSpec as P

TOP_K = 2
MESH = pl.DeviceIdType.MESH
VMEM = pl.BlockSpec(memory_space=pltpu.VMEM)
HBM = pl.BlockSpec(memory_space=pltpu.HBM)

clamp_limit = 7.0
sigmoid_sharpness = 1.702


def contract_rows(left, right):
    return lax.dot_general(
        left, right, (((0,), (0,)), ((), ())), preferred_element_type=jnp.float32
    )


def contract_cols(left, right):
    return lax.dot_general(
        left, right, (((1,), (1,)), ((), ())), preferred_element_type=jnp.float32
    )


def greet(peers, sp, tp):
    barrier = pltpu.get_barrier_semaphore()
    others = [(sp ^ k, tp) for k in range(1, peers)] + [(sp, tp ^ 1), (sp, tp ^ 2)]
    for other in others:
        pl.semaphore_signal(barrier, inc=1, device_id=other, device_id_type=MESH)
    return len(others)


def remote(src, dst, sems, kind, at, device):
    return pltpu.make_async_remote_copy(
        src_ref=src,
        dst_ref=dst,
        send_sem=sems.at[(2 * kind,) + at],
        recv_sem=sems.at[(2 * kind + 1,) + at],
        device_id=device,
        device_id_type=MESH,
    )


def peer_groups(peers):
    cut = max(peers // 2, 1)
    near, far = list(range(1, cut)), list(range(cut, peers))
    quarter = peers // 4
    first = [0] + near[: max(quarter - 1, 0)] + far[:quarter]
    second = near[max(quarter - 1, 0) :] + far[quarter:]
    return first, second


def arrival_order(peers):
    cut = max(peers // 2, 1)
    near, far = list(range(1, cut)), list(range(cut, peers))
    return near[:2] + far[:1] + near[2:] + far[1:]


def gather_order(peers):
    order = [0]
    bit = peers // 2
    while bit:
        order = order + [k ^ bit for k in order]
        bit //= 2
    return order


def layer_kernel(peers, parts, cap, head_dim, names, *refs):
    r = types.SimpleNamespace(**dict(zip(names, refs, strict=True)))
    wg, wu, wd, xr, gr, sx, sg = r.wg, r.wu, r.wd, r.xr, r.gr, r.sx, r.sg
    act, gg, ug, part, comb = r.act, r.gg, r.ug, r.part, r.comb
    pre_g, pre_u, pre_a = r.pre_g, r.pre_u, r.pre_a
    rx1, acc, sb, rx2, ret = r.rx1, r.acc, r.sb, r.rx2, r.ret
    mixbuf, res = r.mixbuf, r.res
    dsems, rsems, tsems, msems, lsems = r.dsems, r.rsems, r.tsems, r.msems, r.lsems
    sp, tp = lax.axis_index("sp"), lax.axis_index("tp")
    tokens, width = r.xs.shape
    x_full = width * parts
    sets = peer_groups(peers)
    steps = sets[0] + sets[1]
    half = len(sets[0])
    groups = [list(range(half)), list(range(half, peers))]
    arrivals = [steps.index(k) for k in arrival_order(peers)]
    outgoing = list(arrivals)

    def far_first(g):
        return sorted(groups[g], key=lambda j: (steps[j] < peers // 2, steps[j]))

    f32, bf16 = jnp.float32, jnp.bfloat16

    def cols(t):
        return pl.ds(pl.multiple_of(t * width, width), width)

    loads = {}
    sources = (
        (r.x_hbm.at[:, cols(tp)], r.xs),
        (r.cot_hbm.at[:, cols(tp)], r.cs),
        (r.routes_hbm, r.routes_ref),
        (r.weights_hbm, r.weights_ref),
        (r.logs_hbm, r.logs_ref),
        (r.mix_hbm, r.mixbuf.at[pl.ds(0, tokens)]),
        (r.q_hbm, r.q_ref),
        (r.k_hbm, r.k_ref),
        (r.v_hbm, r.v_ref),
        (r.states_hbm, r.states_ref),
        (r.gate_hbm, wg),
        (r.up_hbm, wu),
        (r.down_hbm, wd),
        (r.out_hbm, r.wo),
    )
    for i, (src, dst) in enumerate(sources):
        loads[i] = pltpu.make_async_copy(src, dst, lsems.at[i])
        loads[i].start()
    others = greet(peers, sp, tp)
    scope = jax.named_scope

    def rows(j):
        return pl.ds(j * cap, cap)

    with scope("first"):
        loads[2].wait()
        loads[3].wait()
    lane = lax.broadcasted_iota(jnp.int32, (1, 128), 1)
    column = lax.broadcasted_iota(jnp.int32, (128, 1), 0)
    expert = jnp.full((128, 1), -1, jnp.int32)
    for j, k in enumerate(steps):
        expert = jnp.where(column == j, sp ^ k, expert)
    first = r.routes_ref[0:1, :] == expert
    second = r.routes_ref[1:2, :] == expert
    hits = jnp.where(first, 1.0, jnp.where(second, 1.0, 0.0))
    weight_t = jnp.where(
        first, r.weights_ref[0:1, :], jnp.where(second, r.weights_ref[1:2, :], 0.0)
    )
    earlier = jnp.where(
        lax.broadcasted_iota(jnp.int32, (tokens, tokens), 0)
        < lax.broadcasted_iota(jnp.int32, (tokens, tokens), 1),
        1.0,
        0.0,
    ).astype(bf16)
    rank = jnp.dot(hits.astype(bf16), earlier, preferred_element_type=f32)
    place_t = jnp.where(hits > 0.5, rank, -1.0)

    for i in range(2):
        loads[i].wait()
    x_share = r.xs[...]
    c_share = r.cs[...]
    slot = lax.broadcasted_iota(jnp.int32, (cap, tokens), 0).astype(f32)
    firsts, crossings, partners, forwards = {}, {}, {}, {}
    arrays = ((sx, xr), (sg, gr))

    def spread(j):
        k = steps[j]
        here = place_t[j : j + 1, :] == slot
        pick = jnp.where(here, 1.0, 0.0)
        scale = jnp.sum(jnp.where(here, weight_t[j : j + 1, :], 0.0), axis=1, keepdims=True)
        pick = pick.astype(bf16)
        xs = jnp.dot(pick, x_share, preferred_element_type=f32).astype(bf16)
        gs = (jnp.dot(pick, c_share, preferred_element_type=f32) * scale).astype(bf16)
        if k == 0:
            xr[rows(j), cols(tp)] = xs
            gr[rows(j), cols(tp)] = gs
            pass_on(j)
        else:
            sx[rows(j), :] = xs
            sg[rows(j), :] = gs
            for a, (src, dst) in enumerate(arrays):
                copy = remote(
                    src.at[rows(j)], dst.at[rows(j), cols(tp)], dsems, 0, (a, j), (sp ^ k, tp)
                )
                copy.start()
                firsts[a, j] = copy

    def pass_on(j):
        for a, (_, dst) in enumerate(arrays):
            if steps[j]:
                firsts[a, j].wait_recv()
            here = dst.at[rows(j), cols(tp)]
            crossings[a, j] = remote(here, here, dsems, 1, (a, j), (sp, tp ^ 2))
            crossings[a, j].start()
            partners[a, j] = remote(here, here, dsems, 2, (a, j), (sp, tp ^ 1))
            partners[a, j].start()

    def forward(j):
        for a, (_, dst) in enumerate(arrays):
            crossings[a, j].wait_recv()
            here = dst.at[rows(j), cols(tp ^ 2)]
            forwards[a, j] = remote(here, here, dsems, 3, (a, j), (sp, tp ^ 1))
            forwards[a, j].start()

    def arrive(j):
        for a in range(2):
            partners[a, j].wait_recv()
            forwards[a, j].wait_recv()

    def span(g):
        return pl.ds(groups[g][0] * cap, len(groups[g]) * cap)

    def expert_pre(g):
        size = len(groups[g]) * cap
        mine = pl.ds(0, size)
        base = groups[g][0] * cap
        pre_g[mine, :] = jnp.dot(xr[span(g), :], wg[...], preferred_element_type=f32)
        pre_u[mine, :] = jnp.dot(xr[span(g), :], wu[...], preferred_element_type=f32)
        pre_a[mine, :] = contract_cols(gr[span(g), :], wd[...])

        def body(i, carry):
            at = pl.ds(pl.multiple_of(i * 16, 16), 16)
            to = pl.ds(pl.multiple_of(base + i * 16, 16), 16)
            gate_pre, up_pre, act_grad = pre_g[at, :], pre_u[at, :], pre_a[at, :]
            clamped = jnp.minimum(gate_pre, clamp_limit)
            logistic = jax.nn.sigmoid(sigmoid_sharpness * clamped)
            linear = jnp.clip(up_pre, -clamp_limit, clamp_limit)
            swish = clamped * logistic
            act[to, :] = (swish * (linear + 1.0)).astype(bf16)
            slope = logistic + sigmoid_sharpness * swish * (1.0 - logistic)
            gg[to, :] = jnp.where(
                gate_pre < clamp_limit, act_grad * (linear + 1.0) * slope, 0.0
            ).astype(bf16)
            ug[to, :] = jnp.where(
                jnp.abs(up_pre) < clamp_limit, act_grad * swish, 0.0
            ).astype(bf16)
            return carry

        lax.fori_loop(0, size // 16, body, 0)

    def expert_part(g, t):
        part[span(g), cols(t)] = (
            contract_cols(gg[span(g), :], wg[cols(t), :])
            + contract_cols(ug[span(g), :], wu[cols(t), :])
        ).astype(bf16)

    backs, overs, homes = {}, {}, {}

    def back(g, which):
        t = (tp ^ 1, tp ^ 3)[which]
        expert_part(g, t)
        for j in groups[g]:
            copy = remote(
                part.at[rows(j), cols(t)], rx1.at[which, rows(j)], rsems, which, (j,), (sp, tp ^ 1)
            )
            copy.start()
            backs[which, j] = copy

    def cross(j):
        backs[1, j].wait_recv()
        sb[rows(j), :] = (
            part[rows(j), cols(tp ^ 2)].astype(f32) + rx1[1, rows(j), :].astype(f32)
        ).astype(bf16)
        overs[j] = remote(sb.at[rows(j)], rx2.at[rows(j)], rsems, 2, (j,), (sp, tp ^ 2))
        overs[j].start()

    def settle(j):
        backs[0, j].wait_recv()
        acc[rows(j), :] = part[rows(j), cols(tp)].astype(f32) + rx1[0, rows(j), :].astype(f32)

    def home(j):
        k = steps[j]
        overs[j].wait()
        final = (acc[rows(j), :] + rx2[rows(j), :].astype(f32)).astype(bf16)
        if k:
            sb[rows(j), :] = final
            homes[j] = remote(sb.at[rows(j)], ret.at[rows(j)], rsems, 3, (j,), (sp ^ k, tp))
            homes[j].start()
        else:
            ret[rows(j), :] = final

    def block(m):
        return pl.ds(m * tokens, tokens)

    bits = []
    bit = peers // 2
    while bit:
        bits.append(bit)
        bit //= 2
    gathers = {}

    def mix_send(name, at, low, count, to, where):
        gathers[name] = pltpu.make_async_remote_copy(
            src_ref=mixbuf.at[pl.ds(low * tokens, count * tokens)],
            dst_ref=mixbuf.at[pl.ds(to * tokens, count * tokens)],
            send_sem=msems.at[0, at],
            recv_sem=msems.at[1, at],
            device_id=(sp ^ where, tp),
            device_id_type=MESH,
        )
        gathers[name].start()

    here_already = set()

    def mix_block(m, i):
        if m and m not in here_already:
            top = m.bit_length() - 1
            gathers[m - (1 << top), top].wait_recv()
            here_already.add(m)
        to = m + (1 << i)
        mix_send((m, i), to, m, 1, to, bits[i])

    def mix_blocks(chosen):
        for i in range(len(bits)):
            for m in range(1 << i):
                if chosen(m, i) and (m, i) not in gathers:
                    mix_block(m, i)

    with scope("greet"):
        pl.semaphore_wait(pltpu.get_barrier_semaphore(), others)
    queue = list(outgoing)
    with scope("spread"):
        spread(0)
        for j in [queue.pop(0) for _ in range(min(3, len(queue)))]:
            spread(j)
    with scope("comb"):
        size = peers * cap
        slot_at = lax.broadcasted_iota(jnp.int32, (128, size), 1)
        start_at = lax.broadcasted_iota(jnp.int32, (128, size), 0) * cap
        within = (slot_at >= start_at) & (slot_at < start_at + cap)
        member = jnp.where(within, 1.0, 0.0)
        offset = jnp.sum(
            jnp.where(within, (slot_at - start_at).astype(f32), 0.0), axis=0, keepdims=True
        )
        comb[...] = jnp.where(
            jnp.dot(place_t.T.astype(bf16), member.astype(bf16), preferred_element_type=f32)
            == offset,
            1.0,
            0.0,
        ).astype(bf16)

    last = 0
    done = 0
    for i, j in enumerate(arrivals):
        if i == 1:
            with scope("prep"):
                for c in range(4, 10):
                    loads[c].wait()
                mix_blocks(lambda m, i: i == len(bits) - 1 and not m)
                ready = retention_prepare(r, peers, sp, tp, head_dim)
        while j in queue:
            spread(queue.pop(0))
        with scope(f"pass{steps[j]}"):
            pass_on(j)
        if queue and steps[j] != peers // 2:
            spread(queue.pop(0))
        with scope(f"fwd{steps[last]}"):
            forward(last)
        last = j
        done = i + 1
        if all(k in arrivals[:done] for k in groups[0][1:]):
            break
    with scope(f"fwd{steps[last]}"):
        forward(last)
    for j in queue:
        spread(j)
    rest = arrivals[done:]
    early = max(len(rest) - 1, 0)
    for j in rest[:early]:
        with scope(f"pass{steps[j]}"):
            pass_on(j)
    with scope("arrive0"):
        for j in groups[0]:
            arrive(j)
        for i in range(10, 13):
            loads[i].wait()
    mix_blocks(lambda m, i: m == 0 and i)
    with scope("pre0"):
        expert_pre(0)
    for j in rest[early:-1]:
        with scope(f"pass{steps[j]}"):
            pass_on(j)
    with scope("back0"):
        back(0, 1)
        back(0, 0)
    with scope("fwds"):
        for j in rest[:early]:
            forward(j)
    with scope("part0"):
        expert_part(0, tp ^ 2)
        expert_part(0, tp)
    with scope("passz"):
        pass_on(rest[-1])
    with scope("fwdy"):
        mix_blocks(lambda m, i: m == 0)
        for j in rest[early:-1]:
            forward(j)
    with scope("cross0"):
        for j in far_first(0):
            cross(j)
        for j in groups[0]:
            settle(j)
    with scope("fwdz"):
        forward(rest[-1])
    with scope("arrive1"):
        for j in groups[1]:
            arrive(j)
    with scope("pre1"):
        expert_pre(1)
    with scope("home0"):
        for j in far_first(0):
            home(j)
    with scope("mix1"):
        mix_blocks(lambda m, i: m % 2 == 0 or m == 1)
    with scope("back1"):
        back(1, 1)
        back(1, 0)
    with scope("part1"):
        expert_part(1, tp ^ 2)
        expert_part(1, tp)
    with scope("cross1"):
        for j in far_first(1):
            cross(j)
        for j in groups[1]:
            settle(j)
    turns = list(range(8))

    def turn(count):
        for i in turns[:count]:
            wide = x_full // 8
            at = slice(i * wide, (i + 1) * wide)
            r.xt[at, :] = xr[:, at].T
        del turns[:count]

    for i, j in enumerate(far_first(1)):
        with scope("turn"):
            turn(2)
        with scope(f"home{steps[j]}"):
            home(j)
    with scope("turn"):
        turn(len(turns))
        r.act_t[...] = act[...].T
    with scope("total"):
        total = r.cs[...].astype(f32)
        for g in range(2):
            for j in far_first(g):
                if steps[j]:
                    homes[j].wait_recv()
            total = total + jnp.dot(
                comb[:, groups[g][0] * cap : (groups[g][-1] + 1) * cap],
                ret[span(g), :],
                preferred_element_type=f32,
            )
        res[:, cols(tp)] = total.astype(bf16)
    with scope("tail"):
        tails = {}
        cut = tokens // 2

        def of(h, t):
            return res.at[pl.ds(h * cut, cut), cols(t)]

        for h in range(2):
            mine = of(h, tp)
            tails["across", h] = remote(mine, mine, tsems, 0, (h,), (sp, tp ^ 2))
            tails["across", h].start()
            tails["beside", h] = remote(mine, mine, tsems, 1, (h,), (sp, tp ^ 1))
            tails["beside", h].start()
        mix_blocks(lambda m, i: True)
        for h in range(2):
            tails["across", h].wait_recv()
            theirs = of(h, tp ^ 2)
            tails["onward", h] = remote(theirs, theirs, tsems, 2, (h,), (sp, tp ^ 1))
            tails["onward", h].start()
        for h in range(2):
            tails["beside", h].wait_recv()
        for h in range(2):
            tails["onward", h].wait_recv()
        loads[13].wait()

    share = tokens // parts
    piece = res.shape[1] // peers
    order = gather_order(peers)
    where_of = {k: m for m, k in enumerate(order)}
    moved = {}

    def tokens_of(t):
        return pl.ds(pl.multiple_of(t * share, share), share)

    def landing(k, t):
        at = where_of[k] * tokens + t * share
        return r.ares.at[pl.ds(pl.multiple_of(at, share), share)]

    if piece % 128:
        for i in range(peers):
            r.cut[i] = res[:, i * piece : (i + 1) * piece]

    def slice_for(s, t):
        if piece % 128:
            return r.cut.at[s, tokens_of(t)]
        return res.at[tokens_of(t), pl.ds(pl.multiple_of(s * piece, piece), piece)]

    def slice_out(k):
        if k:
            moved[0, k] = remote(
                slice_for(sp ^ k, tp), landing(k, tp), r.fsems, 0, (k,), (sp ^ k, tp)
            )
        else:
            moved[0, k] = pltpu.make_async_copy(slice_for(sp, tp), landing(0, tp), r.fsems.at[0, 0])
        moved[0, k].start()

    def slice_on(k):
        if k:
            moved[0, k].wait_recv()
        else:
            moved[0, k].wait()
        here = landing(k, tp)
        moved[1, k] = remote(here, here, r.fsems, 1, (k,), (sp, tp ^ 2))
        moved[1, k].start()
        moved[2, k] = remote(here, here, r.fsems, 2, (k,), (sp, tp ^ 1))
        moved[2, k].start()

    def slice_forward(k):
        moved[1, k].wait_recv()
        here = landing(k, tp ^ 2)
        moved[3, k] = remote(here, here, r.fsems, 3, (k,), (sp, tp ^ 1))
        moved[3, k].start()

    with scope("slices"):
        for k in steps:
            slice_out(k)
    with scope("gradmix"):
        r.gm[...] = jnp.dot(res[...], r.wo[...], preferred_element_type=f32).astype(bf16)
    scan = Scan(r, peers, sp, tp, head_dim, ready)
    with scope("totals"):
        scan.begin()
    units = [(n, p) for n in range(scan.blocks) for p in range(scan.pairs)]
    rounds = len(bits)
    events = [functools.partial(scan.advance, i) for i in range(rounds)]
    per = -(-len(units) // (rounds + 1))
    todo = [units[i : i + per] for i in range(0, len(units), per)]
    later = [list(range(max(peers // 2, 1))), list(range(max(peers // 2, 1), peers))]
    if rounds == 1:
        later = [later[0] + later[1]]
    later = later + [[]] * (rounds - len(later))
    for i in range(rounds):
        with scope(f"unit{i}"):
            for n, p in todo[i] if i < len(todo) else ():
                scan.unit(n, p)
        with scope(f"scan{i}"):
            events[i]()
        with scope(f"slice_on{i}"):
            for k in later[i]:
                slice_on(k)
            for k in later[i - 1] if i else ():
                slice_forward(k)
    with scope("unitz"):
        for some in todo[rounds:]:
            for n, p in some:
                scan.unit(n, p)
    with scope("finish"):
        scan.finish()
    with scope("slicez"):
        for k in later[-1] if rounds <= 2 else ():
            slice_forward(k)
        for k in steps:
            moved[2, k].wait_recv()
            moved[3, k].wait_recv()
    with scope("mixend"):
        for m in range(peers // 2):
            gathers[m, len(bits) - 1].wait_recv()
    with scope("gradout"):
        r.d_out[...] = contract_rows(r.ares[...], mixbuf[...])
    for group in (firsts, crossings, partners, forwards, backs, homes, gathers):
        for copy in group.values():
            copy.wait_send()
    for key, copy in moved.items():
        if key != (0, 0):
            copy.wait_send()
    for copy in tails.values():
        copy.wait_send()
    scan.close()


def lanes_of(head_dim):
    lane = lax.broadcasted_iota(jnp.int32, (1, 128), 1)
    return [(lane >= a * head_dim) & (lane < (a + 1) * head_dim) for a in range(128 // head_dim)]


def block_mask(head_dim):
    row = lax.broadcasted_iota(jnp.int32, (128, 128), 0)
    lane = lax.broadcasted_iota(jnp.int32, (128, 128), 1)
    mask = jnp.zeros((128, 128), jnp.float32)
    for a in range(128 // head_dim):
        low, high = a * head_dim, (a + 1) * head_dim
        inside = (row >= low) & (row < high) & (lane >= low) & (lane < high)
        mask = jnp.where(inside, 1.0, mask)
    return mask


def stacked(values, head_dim):
    keep = [jnp.where(m, 1.0, 0.0).astype(jnp.bfloat16) for m in lanes_of(head_dim)]
    return jnp.concatenate([values * m for m in keep], axis=0)


def retention_prepare(r, peers, sp, tp, head_dim):
    f32, bf16 = jnp.float32, jnp.bfloat16
    heads, tokens = r.logs_ref.shape
    pairs = r.q_ref.shape[1] // 128
    per = 128 // head_dim
    blocks = r.states_ref.shape[0] // (heads * head_dim)
    size = tokens // blocks
    picks = lanes_of(head_dim)
    row = lax.broadcasted_iota(jnp.int32, (size, size), 0)
    col = lax.broadcasted_iota(jnp.int32, (size, size), 1)
    upto = jnp.where(row <= col, 1.0, 0.0).astype(bf16)
    causal = row >= col
    logs = r.logs_ref[...]
    high = logs.astype(bf16).astype(f32)
    middle = (logs - high).astype(bf16).astype(f32)
    low = logs - high - middle
    split = jnp.concatenate([high, middle, low], axis=0).astype(bf16)
    spare = jnp.zeros((128 - heads, size), f32)

    def expand(values, p):
        out = values[:, p * per : p * per + 1]
        for a in range(1, per):
            out = jnp.where(picks[a], values[:, p * per + a : p * per + a + 1], out)
        return jnp.where(picks[0], values[:, p * per : p * per + 1], out)

    before = jnp.zeros((1, 128), f32)
    tile = jnp.zeros((head_dim, 128), f32)
    d_at = lax.broadcasted_iota(jnp.int32, (head_dim, 128), 0)
    l_at = lax.broadcasted_iota(jnp.int32, (head_dim, 128), 1)
    for a in range(per):
        tile = jnp.where(l_at == d_at + a * head_dim, 1.0, tile)
    tile = tile.astype(bf16)
    diagonal = block_mask(head_dim)
    for n in range(blocks):
        at = slice(n * size, (n + 1) * size)
        sums = jnp.dot(split[:, at], upto, preferred_element_type=f32)
        cum_t = sums[:heads] + sums[heads : 2 * heads] + sums[2 * heads :]
        cum = jnp.concatenate([cum_t, spare], axis=0).T
        end = cum[size - 1 : size, :]
        from_start = jnp.exp(cum)
        to_end = jnp.exp(end - cum)
        from_device = jnp.exp(cum + before)
        end_factor = jnp.exp(end)
        before = before + end
        for p in range(pairs):
            u = n * pairs + p
            lanes = slice(p * 128, (p + 1) * 128)
            q = r.q_ref[at, lanes]
            k = r.k_ref[at, lanes]
            begin = expand(from_start, p)
            r.fs[at, lanes] = begin
            r.te[at, lanes] = expand(to_end, p)
            r.rq[at, lanes] = (q.astype(f32) * begin).astype(bf16)
            r.tq[at, lanes] = (q.astype(f32) * expand(from_device, p)).astype(bf16)
            r.ends[n, p : p + 1, :] = expand(end_factor, p)
            for a in range(per):
                h = p * per + a
                gap = cum[:, h : h + 1] - cum_t[h : h + 1, :]
                r.dec[u, a * size : (a + 1) * size, :] = jnp.where(
                    causal, jnp.exp(jnp.minimum(gap, 0.0)), 0.0
                )
            score = contract_cols(stacked(q, head_dim), k)
            r.ws[u] = (score * r.dec[u]).astype(bf16)
            start = (n * heads + p * per) * head_dim
            states = r.states_ref[start : start + 128, :]
            wide = jnp.dot(states, tile, preferred_element_type=f32)
            r.stbd[u] = (wide * diagonal).astype(bf16)
    for p in range(pairs):
        r.own_log[p : p + 1, :] = expand(before, p)
    for p in range(pairs, 8):
        r.own_log[p : p + 1, :] = jnp.zeros((1, 128), f32)
    r.all_logs[sp] = r.own_log[...]
    copies = []
    for k in range(1, peers):
        copy = remote(r.own_log, r.all_logs.at[sp], r.gsems, 0, (k,), (sp ^ k, tp))
        copy.start()
        copies.append(copy)
    return copies


class Scan:
    def __init__(self, r, peers, sp, tp, head_dim, logs):
        self.r, self.peers, self.sp, self.tp, self.head_dim = r, peers, sp, tp, head_dim
        heads = r.logs_ref.shape[0]
        self.pairs = r.q_ref.shape[1] // 128
        self.per = 128 // head_dim
        self.blocks = r.states_ref.shape[0] // (heads * head_dim)
        self.size = r.logs_ref.shape[1] // self.blocks
        self.logs = logs
        self.sent = []

    def fold(self, full):
        full = full * block_mask(self.head_dim)
        out = full[: self.head_dim]
        for a in range(1, self.per):
            out = out + full[a * self.head_dim : (a + 1) * self.head_dim]
        return out

    def rows(self, p):
        return slice(p * self.head_dim, (p + 1) * self.head_dim)

    def begin(self):
        r = self.r
        for p in range(self.pairs):
            lanes = slice(p * 128, (p + 1) * 128)
            r.tot[self.rows(p), :] = self.fold(contract_rows(r.tq[:, lanes], r.gm[:, lanes]))
        r.suffix[...] = jnp.zeros(r.suffix.shape, jnp.float32)
        self.push(0)
        for copy in self.logs:
            copy.wait_recv()

    def push(self, i):
        r = self.r
        r.tsend[i] = r.tot[...].astype(jnp.bfloat16)
        copy = remote(
            r.tsend.at[i], r.trecv.at[i], r.ssems, 0, (i,), (self.sp ^ (1 << i), self.tp)
        )
        copy.start()
        self.sent.append(copy)

    def advance(self, i):
        r, sp, b = self.r, self.sp, 1 << i
        lower = (sp // b) % 2 == 0
        mine, base = sp // b, (sp // (2 * b)) * 2
        reach = jnp.zeros((8, 128), jnp.float32)
        group = jnp.zeros((8, 128), jnp.float32)
        for m in range(self.peers):
            ahead = jnp.where(jnp.logical_and(sp < m, mine == m // b), 1.0, 0.0)
            reach = reach + ahead * r.all_logs[m]
            group = group + jnp.where(base == m // b, 1.0, 0.0) * r.all_logs[m]
        up = jnp.where(lower, 1.0, 0.0)
        reach = jnp.exp(reach) * up
        group = jnp.exp(group)
        self.sent[i].wait_recv()
        for p in range(self.pairs):
            at = self.rows(p)
            mine_t = r.tot[at, :]
            theirs = r.trecv[i, at, :].astype(jnp.float32)
            r.suffix[at, :] = r.suffix[at, :] + reach[p : p + 1, :] * theirs
            early = up * mine_t + (1.0 - up) * theirs
            late = up * theirs + (1.0 - up) * mine_t
            r.tot[at, :] = early + group[p : p + 1, :] * late
        if 2 * b < self.peers:
            self.push(i + 1)

    def unit(self, n, p):
        r, size = self.r, self.size
        f32, bf16 = jnp.float32, jnp.bfloat16
        at = slice(n * size, (n + 1) * size)
        lanes = slice(p * 128, (p + 1) * 128)
        u = n * self.pairs + p
        g, v, k, q = r.gm[at, lanes], r.v_ref[at, lanes], r.k_ref[at, lanes], r.q_ref[at, lanes]
        grads = stacked(g, self.head_dim)
        weighted = (contract_cols(grads, v) * r.dec[u]).astype(bf16)
        wide = jnp.concatenate(
            [weighted[a * size : (a + 1) * size] for a in range(self.per)], axis=1
        )
        intra = jnp.dot(wide, stacked(k, self.head_dim), preferred_element_type=f32)
        carry = contract_cols(g, r.stbd[u])
        r.gq[at, lanes] = (intra + carry * r.fs[at, lanes]).astype(bf16)
        r.ki[at, lanes] = contract_rows(weighted, stacked(q, self.head_dim))
        r.vi[at, lanes] = contract_rows(r.ws[u], grads)
        r.outer[n, self.rows(p), :] = self.fold(contract_rows(r.rq[at, lanes], g))

    def finish(self):
        r, size = self.r, self.size
        bf16 = jnp.bfloat16
        diagonal = block_mask(self.head_dim)
        for p in range(self.pairs):
            lanes = slice(p * 128, (p + 1) * 128)
            state = r.suffix[self.rows(p), :]
            for n in reversed(range(self.blocks)):
                at = slice(n * size, (n + 1) * size)
                rounded = state.astype(bf16).astype(jnp.float32)
                full = (jnp.concatenate([rounded] * self.per, axis=0) * diagonal).astype(bf16)
                v, k = r.v_ref[at, lanes], r.k_ref[at, lanes]
                te = r.te[at, lanes]
                r.gk[at, lanes] = (r.ki[at, lanes] + contract_cols(v, full) * te).astype(bf16)
                r.gv[at, lanes] = (
                    r.vi[at, lanes] + jnp.dot(k, full, preferred_element_type=jnp.float32) * te
                ).astype(bf16)
                if n:
                    state = r.ends[n, p : p + 1, :] * state + r.outer[n, self.rows(p), :]

    def close(self):
        for copy in self.logs + self.sent:
            copy.wait_send()


def layer_backward(arrays, peers, parts, capacity, head_dim):
    cap = -(-capacity // 16) * 16
    tokens, full = arrays["x_hbm"].shape
    hidden = arrays["gate_hbm"].shape[1]
    local = arrays["q_hbm"].shape[1]
    blocks = arrays["states_hbm"].shape[0] // local
    size = tokens // blocks
    pairs = local // 128
    units = blocks * pairs
    width = full // parts
    piece = full // peers
    total = peers * cap
    most = max(len(g) for g in peer_groups(peers)) * cap
    bits = peers.bit_length() - 1
    bf16, f32 = jnp.bfloat16, jnp.float32

    def shape(*dims, dtype=bf16):
        return jax.ShapeDtypeStruct(dims, dtype)

    def vmem(*dims, dtype=bf16):
        return pltpu.VMEM(dims, dtype)

    outs = dict(
        xt=shape(full, total),
        gr=shape(total, full),
        act_t=shape(hidden, total),
        gg=shape(total, hidden),
        ug=shape(total, hidden),
        d_out=shape(piece, local, dtype=f32),
        gq=shape(tokens, local),
        gk=shape(tokens, local),
        gv=shape(tokens, local),
    )
    scratch = dict(
        ares=vmem(peers * tokens, piece),
        mixbuf=vmem(peers * tokens, local),
        xs=vmem(tokens, width),
        cs=vmem(tokens, width),
        q_ref=vmem(tokens, local),
        k_ref=vmem(tokens, local),
        v_ref=vmem(tokens, local),
        routes_ref=vmem(*arrays["routes_hbm"].shape, dtype=jnp.int32),
        weights_ref=vmem(*arrays["weights_hbm"].shape, dtype=f32),
        logs_ref=vmem(*arrays["logs_hbm"].shape, dtype=f32),
        states_ref=vmem(*arrays["states_hbm"].shape),
        wg=vmem(full, hidden),
        wu=vmem(full, hidden),
        wd=vmem(hidden, full),
        wo=vmem(full, local),
        xr=vmem(total, full),
        sx=vmem(total, width),
        sg=vmem(total, width),
        pre_g=vmem(most, hidden, dtype=f32),
        pre_u=vmem(most, hidden, dtype=f32),
        pre_a=vmem(most, hidden, dtype=f32),
        act=vmem(total, hidden),
        part=vmem(total, full),
        rx1=vmem(2, total, width),
        acc=vmem(total, width, dtype=f32),
        sb=vmem(total, width),
        rx2=vmem(total, width),
        ret=vmem(total, width),
        comb=vmem(tokens, total),
        res=vmem(tokens, full),
        gm=vmem(tokens, local),
        rq=vmem(tokens, local),
        tq=vmem(tokens, local),
        fs=vmem(tokens, local, dtype=f32),
        te=vmem(tokens, local, dtype=f32),
        ki=vmem(tokens, local, dtype=f32),
        vi=vmem(tokens, local, dtype=f32),
        dec=vmem(units, 128 // head_dim * size, size, dtype=f32),
        ws=vmem(units, 128 // head_dim * size, size),
        stbd=vmem(units, 128, 128),
        ends=vmem(blocks, 8, 128, dtype=f32),
        own_log=vmem(8, 128, dtype=f32),
        all_logs=vmem(peers, 8, 128, dtype=f32),
        tot=vmem(pairs * head_dim, 128, dtype=f32),
        suffix=vmem(pairs * head_dim, 128, dtype=f32),
        outer=vmem(blocks, pairs * head_dim, 128, dtype=f32),
        tsend=vmem(bits, pairs * head_dim, 128),
        trecv=vmem(bits, pairs * head_dim, 128),
        dsems=pltpu.SemaphoreType.DMA((8, 2, peers)),
        rsems=pltpu.SemaphoreType.DMA((8, peers)),
        tsems=pltpu.SemaphoreType.DMA((6, 2)),
        msems=pltpu.SemaphoreType.DMA((2, peers)),
        lsems=pltpu.SemaphoreType.DMA((14,)),
        fsems=pltpu.SemaphoreType.DMA((8, peers)),
        gsems=pltpu.SemaphoreType.DMA((2, peers)),
        ssems=pltpu.SemaphoreType.DMA((2, bits)),
    )
    if piece % 128:
        scratch["cut"] = vmem(peers, tokens, piece)
    names = list(arrays) + list(outs) + list(scratch)

    def place(name, value):
        if name.endswith("hbm"):
            return pltpu.with_memory_space_constraint(value, pltpu.HBM)
        return value

    results = pl.pallas_call(
        functools.partial(layer_kernel, peers, parts, cap, head_dim, names),
        out_shape=tuple(outs.values()),
        in_specs=[HBM if name.endswith("hbm") else VMEM for name in arrays],
        out_specs=(VMEM,) * len(outs),
        scratch_shapes=list(scratch.values()),
        compiler_params=pltpu.CompilerParams(
            collective_id=0, has_side_effects=True, vmem_limit_bytes=(42 if peers <= 8 else 63) * 2**20
        ),
        name="layer_backward",
    )(*[place(name, value) for name, value in arrays.items()])
    return weight_grads(*results)


def weights_kernel(
    xt, g, act, gg, ug, i_out, i_q, i_k, i_v,
    d_gate, d_up, d_down, d_out, o_q, o_k, o_v,
    v_gate, v_up, v_down, osems,
):
    full = v_gate.shape[0]
    count, parts = 8, 4
    wide, broad = full // count, full // parts
    f32 = jnp.float32
    stores = []

    def store(src, dst):
        copy = pltpu.make_async_copy(src, dst, osems.at[len(stores)])
        copy.start()
        stores.append(copy)

    for i in range(count):
        at = slice(i * wide, (i + 1) * wide)
        v_gate[at, :] = jnp.dot(xt[at, :], gg[...], preferred_element_type=f32)
        store(v_gate.at[at], d_gate.at[at])
        v_up[at, :] = jnp.dot(xt[at, :], ug[...], preferred_element_type=f32)
        store(v_up.at[at], d_up.at[at])
    for src, dst in ((i_out, d_out), (i_q, o_q), (i_k, o_k), (i_v, o_v)):
        store(src, dst)
    for i in range(parts):
        at = slice(i * broad, (i + 1) * broad)
        v_down[:, at] = jnp.dot(act[...], g[:, at], preferred_element_type=f32)
        store(v_down.at[:, at], d_down.at[:, at])
    for copy in stores:
        copy.wait()


def weight_grads(xt, g, act, gg, ug, d_out, q, k, v):
    full, total = xt.shape
    hidden = act.shape[0]
    f32 = jnp.float32
    grads = [jax.ShapeDtypeStruct(s, f32) for s in ((full, hidden), (full, hidden), (hidden, full))]
    others = [jax.ShapeDtypeStruct(a.shape, a.dtype) for a in (d_out, q, k, v)]
    limit = 62 if total > 640 else 20
    return pl.pallas_call(
        weights_kernel,
        out_shape=tuple(grads + others),
        in_specs=[VMEM] * 9,
        out_specs=(HBM,) * 7,
        scratch_shapes=[pltpu.VMEM(a.shape, a.dtype) for a in grads]
        + [pltpu.SemaphoreType.DMA((24,))],
        compiler_params=pltpu.CompilerParams(vmem_limit_bytes=limit * 2**20),
        name="weight_grads",
    )(xt, g, act, gg, ug, d_out, q, k, v)


def shards(
    moe_input,
    cotangent,
    routes,
    route_weights,
    gate_weight,
    up_weight,
    down_weight,
    out_weight,
    mixer_output,
    queries,
    key_vectors,
    value_vectors,
    log_decay,
    block_states,
):
    tok_dev, model_width = cotangent.shape
    peers, parts = lax.axis_size("sp"), lax.axis_size("tp")
    capacity = 5 * tok_dev * TOP_K // (4 * peers)
    head_dim = block_states.shape[-1]
    arrays = dict(
        routes_hbm=routes.T,
        weights_hbm=route_weights.T,
        x_hbm=moe_input,
        cot_hbm=cotangent,
        gate_hbm=gate_weight[0],
        up_hbm=up_weight[0],
        down_hbm=down_weight[0],
        out_hbm=out_weight,
        mix_hbm=mixer_output,
        q_hbm=queries,
        k_hbm=key_vectors,
        v_hbm=value_vectors,
        logs_hbm=log_decay.T,
        states_hbm=block_states.reshape(-1, head_dim),
    )
    grad_gate, grad_up, grad_down, *others = layer_backward(
        arrays, peers, parts, capacity, head_dim
    )
    return (grad_gate[None], grad_up[None], grad_down[None], *others)


def solution(mesh):
    return jax.shard_map(
        shards,
        mesh=mesh,
        in_specs=(
            P("sp", None),
            P("sp", None),
            P("sp", None),
            P("sp", None),
            P("sp", None, "tp"),
            P("sp", None, "tp"),
            P("sp", "tp", None),
            P(None, "tp"),
            P("sp", "tp"),
            P("sp", "tp"),
            P("sp", "tp"),
            P("sp", "tp"),
            P("sp", "tp"),
            P("sp", "tp", None, None),
        ),
        out_specs=(
            P("sp", None, "tp"),
            P("sp", None, "tp"),
            P("sp", "tp", None),
            P("sp", "tp"),
            P("sp", "tp"),
            P("sp", "tp"),
            P("sp", "tp"),
        ),
        check_vma=False,
    )
```

```python
import functools
import types

import jax
import jax.numpy as jnp
from jax import lax
from jax.experimental import pallas as pl
from jax.experimental.pallas import tpu as pltpu
from jax.sharding import PartitionSpec as P

TOP_K = 2
MESH = pl.DeviceIdType.MESH
VMEM = pl.BlockSpec(memory_space=pltpu.VMEM)
HBM = pl.BlockSpec(memory_space=pltpu.HBM)

clamp_limit = 7.0
sigmoid_sharpness = 1.702


def contract_rows(left, right):
    return lax.dot_general(
        left, right, (((0,), (0,)), ((), ())), preferred_element_type=jnp.float32
    )


def contract_cols(left, right):
    return lax.dot_general(
        left, right, (((1,), (1,)), ((), ())), preferred_element_type=jnp.float32
    )


def greet(peers, sp, tp):
    barrier = pltpu.get_barrier_semaphore()
    others = [(sp ^ k, tp) for k in range(1, peers)] + [(sp, tp ^ 1), (sp, tp ^ 2)]
    for other in others:
        pl.semaphore_signal(barrier, inc=1, device_id=other, device_id_type=MESH)
    return len(others)


def remote(src, dst, sems, kind, at, device):
    return pltpu.make_async_remote_copy(
        src_ref=src,
        dst_ref=dst,
        send_sem=sems.at[(2 * kind,) + at],
        recv_sem=sems.at[(2 * kind + 1,) + at],
        device_id=device,
        device_id_type=MESH,
    )


def peer_groups(peers):
    cut = max(peers // 2, 1)
    near, far = list(range(1, cut)), list(range(cut, peers))
    quarter = peers // 4
    first = [0] + near[: max(quarter - 1, 0)] + far[:quarter]
    second = near[max(quarter - 1, 0) :] + far[quarter:]
    return first, second


def arrival_order(peers):
    cut = max(peers // 2, 1)
    near, far = list(range(1, cut)), list(range(cut, peers))
    return near[:2] + far[:1] + near[2:] + far[1:]


def send_order(peers):
    cut = max(peers // 2, 1)
    near, far = list(range(1, cut)), list(range(cut, peers))
    return near[:2] + far[:2] + near[2:] + far[2:]


def gather_order(peers):
    order = [0]
    bit = peers // 2
    while bit:
        order = order + [k ^ bit for k in order]
        bit //= 2
    return order


def layer_kernel(peers, parts, cap, head_dim, names, *refs):
    r = types.SimpleNamespace(**dict(zip(names, refs, strict=True)))
    wg, wu, wd, xr, gr, sx, sg = r.wg, r.wu, r.wd, r.xr, r.gr, r.sx, r.sg
    act, gg, ug, part, comb = r.act, r.gg, r.ug, r.part, r.comb
    pre_g, pre_u = r.pre_g, r.pre_u
    rx1, acc, sb, rx2, ret = r.rx1, r.acc, r.sb, r.rx2, r.ret
    mixbuf, res = r.mixbuf, r.res
    dsems, rsems, tsems, msems, lsems = r.dsems, r.rsems, r.tsems, r.msems, r.lsems
    sp, tp = lax.axis_index("sp"), lax.axis_index("tp")
    tokens, width = r.xs.shape
    x_full = width * parts
    sets = peer_groups(peers)
    steps = sets[0] + sets[1]
    half = len(sets[0])
    groups = [list(range(half)), list(range(half, peers))]
    arrivals = [steps.index(k) for k in arrival_order(peers)]
    outgoing = [steps.index(k) for k in send_order(peers)]

    def far_first(g):
        return sorted(groups[g], key=lambda j: (steps[j] < peers // 2, steps[j]))

    f32, bf16 = jnp.float32, jnp.bfloat16

    def cols(t):
        return pl.ds(pl.multiple_of(t * width, width), width)

    loads = {}
    sources = (
        (r.x_hbm.at[:, cols(tp)], r.xs),
        (r.cot_hbm.at[:, cols(tp)], r.cs),
        (r.routes_hbm, r.routes_ref),
        (r.weights_hbm, r.weights_ref),
        (r.logs_hbm, r.logs_ref),
        (r.mix_hbm, r.mixbuf.at[pl.ds(0, tokens)]),
        (r.q_hbm, r.q_ref),
        (r.k_hbm, r.k_ref),
        (r.v_hbm, r.v_ref),
        (r.states_hbm, r.states_ref),
        (r.gate_hbm, wg),
        (r.up_hbm, wu),
        (r.down_hbm, wd),
        (r.out_hbm, r.wo),
    )
    for i, (src, dst) in enumerate(sources):
        loads[i] = pltpu.make_async_copy(src, dst, lsems.at[i])
        loads[i].start()
    others = greet(peers, sp, tp)
    scope = jax.named_scope

    def rows(j):
        return pl.ds(j * cap, cap)

    with scope("first"):
        loads[2].wait()
        loads[3].wait()
    lane = lax.broadcasted_iota(jnp.int32, (1, 128), 1)
    column = lax.broadcasted_iota(jnp.int32, (128, 1), 0)
    expert = jnp.full((128, 1), -1, jnp.int32)
    for j, k in enumerate(steps):
        expert = jnp.where(column == j, sp ^ k, expert)
    first = r.routes_ref[0:1, :] == expert
    second = r.routes_ref[1:2, :] == expert
    hits = jnp.where(first, 1.0, jnp.where(second, 1.0, 0.0))
    weight_t = jnp.where(
        first, r.weights_ref[0:1, :], jnp.where(second, r.weights_ref[1:2, :], 0.0)
    )
    earlier = jnp.where(
        lax.broadcasted_iota(jnp.int32, (tokens, tokens), 0)
        < lax.broadcasted_iota(jnp.int32, (tokens, tokens), 1),
        1.0,
        0.0,
    ).astype(bf16)
    rank = jnp.dot(hits.astype(bf16), earlier, preferred_element_type=f32)
    place_t = jnp.where(hits > 0.5, rank, -1.0)

    for i in range(2):
        loads[i].wait()
    x_share = r.xs[...]
    c_share = r.cs[...]
    slot = lax.broadcasted_iota(jnp.int32, (cap, tokens), 0).astype(f32)
    firsts, crossings, partners, forwards = {}, {}, {}, {}
    arrays = ((sx, xr), (sg, gr))

    def spread(j):
        k = steps[j]
        here = place_t[j : j + 1, :] == slot
        pick = jnp.where(here, 1.0, 0.0)
        scale = jnp.sum(jnp.where(here, weight_t[j : j + 1, :], 0.0), axis=1, keepdims=True)
        pick = pick.astype(bf16)
        xs = jnp.dot(pick, x_share, preferred_element_type=f32).astype(bf16)
        gs = (jnp.dot(pick, c_share, preferred_element_type=f32) * scale).astype(bf16)
        if k == 0:
            xr[rows(j), cols(tp)] = xs
            gr[rows(j), cols(tp)] = gs
            pass_on(j)
        else:
            sx[rows(j), :] = xs
            sg[rows(j), :] = gs
            for a, (src, dst) in enumerate(arrays):
                copy = remote(
                    src.at[rows(j)], dst.at[rows(j), cols(tp)], dsems, 0, (a, j), (sp ^ k, tp)
                )
                copy.start()
                firsts[a, j] = copy

    def pass_on(j):
        for a, (_, dst) in enumerate(arrays):
            if steps[j]:
                firsts[a, j].wait_recv()
            here = dst.at[rows(j), cols(tp)]
            crossings[a, j] = remote(here, here, dsems, 1, (a, j), (sp, tp ^ 2))
            crossings[a, j].start()
            partners[a, j] = remote(here, here, dsems, 2, (a, j), (sp, tp ^ 1))
            partners[a, j].start()

    def forward(j):
        for a, (_, dst) in enumerate(arrays):
            crossings[a, j].wait_recv()
            here = dst.at[rows(j), cols(tp ^ 2)]
            forwards[a, j] = remote(here, here, dsems, 3, (a, j), (sp, tp ^ 1))
            forwards[a, j].start()

    def arrive(j):
        for a in range(2):
            partners[a, j].wait_recv()
            forwards[a, j].wait_recv()

    def span(g):
        return pl.ds(groups[g][0] * cap, len(groups[g]) * cap)

    def expert_pre(g):
        size = len(groups[g]) * cap
        mine = pl.ds(0, size)
        base = groups[g][0] * cap
        pre_g[mine, :] = jnp.dot(xr[span(g), :], wg[...], preferred_element_type=f32)
        pre_u[mine, :] = jnp.dot(xr[span(g), :], wu[...], preferred_element_type=f32)
        acc[span(g), :] = contract_cols(gr[span(g), :], wd[...])

        def body(i, carry):
            at = pl.ds(pl.multiple_of(i * 16, 16), 16)
            to = pl.ds(pl.multiple_of(base + i * 16, 16), 16)
            gate_pre, up_pre, act_grad = pre_g[at, :], pre_u[at, :], acc[to, :]
            clamped = jnp.minimum(gate_pre, clamp_limit)
            logistic = jax.nn.sigmoid(sigmoid_sharpness * clamped)
            linear = jnp.clip(up_pre, -clamp_limit, clamp_limit)
            swish = clamped * logistic
            act[to, :] = (swish * (linear + 1.0)).astype(bf16)
            slope = logistic + sigmoid_sharpness * swish * (1.0 - logistic)
            gg[to, :] = jnp.where(
                gate_pre < clamp_limit, act_grad * (linear + 1.0) * slope, 0.0
            ).astype(bf16)
            ug[to, :] = jnp.where(
                jnp.abs(up_pre) < clamp_limit, act_grad * swish, 0.0
            ).astype(bf16)
            return carry

        lax.fori_loop(0, size // 16, body, 0)

    def expert_part(g, t):
        part[span(g), cols(t)] = (
            contract_cols(gg[span(g), :], wg[cols(t), :])
            + contract_cols(ug[span(g), :], wu[cols(t), :])
        ).astype(bf16)

    backs, overs, homes = {}, {}, {}

    def back(g, which):
        t = (tp ^ 1, tp ^ 3)[which]
        expert_part(g, t)
        for j in groups[g]:
            copy = remote(
                part.at[rows(j), cols(t)], rx1.at[which, rows(j)], rsems, which, (j,), (sp, tp ^ 1)
            )
            copy.start()
            backs[which, j] = copy

    def cross(j):
        backs[1, j].wait_recv()
        sb[rows(j), :] = (
            part[rows(j), cols(tp ^ 2)].astype(f32) + rx1[1, rows(j), :].astype(f32)
        ).astype(bf16)
        overs[j] = remote(sb.at[rows(j)], rx2.at[rows(j)], rsems, 2, (j,), (sp, tp ^ 2))
        overs[j].start()

    def settle(j):
        backs[0, j].wait_recv()
        acc[rows(j), :] = part[rows(j), cols(tp)].astype(f32) + rx1[0, rows(j), :].astype(f32)

    def home(j):
        k = steps[j]
        overs[j].wait()
        final = (acc[rows(j), :] + rx2[rows(j), :].astype(f32)).astype(bf16)
        if k:
            sb[rows(j), :] = final
            homes[j] = remote(sb.at[rows(j)], ret.at[rows(j)], rsems, 3, (j,), (sp ^ k, tp))
            homes[j].start()
        else:
            ret[rows(j), :] = final

    def block(m):
        return pl.ds(m * tokens, tokens)

    bits = []
    bit = peers // 2
    while bit:
        bits.append(bit)
        bit //= 2
    gathers = {}

    def mix_send(name, at, low, count, to, where):
        gathers[name] = pltpu.make_async_remote_copy(
            src_ref=mixbuf.at[pl.ds(low * tokens, count * tokens)],
            dst_ref=mixbuf.at[pl.ds(to * tokens, count * tokens)],
            send_sem=msems.at[0, at],
            recv_sem=msems.at[1, at],
            device_id=(sp ^ where, tp),
            device_id_type=MESH,
        )
        gathers[name].start()

    here_already = set()

    def mix_block(m, i):
        if m and m not in here_already:
            top = m.bit_length() - 1
            gathers[m - (1 << top), top].wait_recv()
            here_already.add(m)
        to = m + (1 << i)
        mix_send((m, i), to, m, 1, to, bits[i])

    def mix_blocks(chosen):
        for i in range(len(bits)):
            for m in range(1 << i):
                if chosen(m, i) and (m, i) not in gathers:
                    mix_block(m, i)

    with scope("greet"):
        pl.semaphore_wait(pltpu.get_barrier_semaphore(), others)
    queue = list(outgoing)
    with scope("spread"):
        spread(0)
        for j in [queue.pop(0) for _ in range(min(3, len(queue)))]:
            spread(j)
    with scope("comb"):
        size = peers * cap
        slot_at = lax.broadcasted_iota(jnp.int32, (128, size), 1)
        start_at = lax.broadcasted_iota(jnp.int32, (128, size), 0) * cap
        within = (slot_at >= start_at) & (slot_at < start_at + cap)
        member = jnp.where(within, 1.0, 0.0)
        offset = jnp.sum(
            jnp.where(within, (slot_at - start_at).astype(f32), 0.0), axis=0, keepdims=True
        )
        comb[...] = jnp.where(
            jnp.dot(place_t.T.astype(bf16), member.astype(bf16), preferred_element_type=f32)
            == offset,
            1.0,
            0.0,
        ).astype(bf16)

    last = 0
    done = 0
    for i, j in enumerate(arrivals):
        if i == 1:
            with scope("prep"):
                for c in range(4, 10):
                    loads[c].wait()
                mix_blocks(lambda m, i: i == len(bits) - 1 and not m)
                ready = retention_prepare(r, peers, sp, tp, head_dim)
        while j in queue:
            spread(queue.pop(0))
        with scope(f"pass{steps[j]}"):
            pass_on(j)
        if queue:
            spread(queue.pop(0))
        with scope(f"fwd{steps[last]}"):
            forward(last)
        last = j
        done = i + 1
        if all(k in arrivals[:done] for k in groups[0][1:]):
            break
    with scope(f"fwd{steps[last]}"):
        forward(last)
    for j in queue:
        spread(j)
    rest = arrivals[done:]
    early = max(len(rest) - 1, 0)
    for j in rest[:early]:
        with scope(f"pass{steps[j]}"):
            pass_on(j)
    with scope("arrive0"):
        for j in groups[0]:
            arrive(j)
        for i in range(10, 13):
            loads[i].wait()
    mix_blocks(lambda m, i: m == 0 and i)
    with scope("pre0"):
        expert_pre(0)
    for j in rest[early:-1]:
        with scope(f"pass{steps[j]}"):
            pass_on(j)
    with scope("back0"):
        back(0, 1)
        back(0, 0)
    with scope("fwds"):
        for j in rest[:early]:
            forward(j)
    with scope("part0"):
        expert_part(0, tp ^ 2)
        expert_part(0, tp)
    with scope("passz"):
        pass_on(rest[-1])
    with scope("fwdy"):
        mix_blocks(lambda m, i: m == 0)
        for j in rest[early:-1]:
            forward(j)
    with scope("cross0"):
        for j in far_first(0):
            cross(j)
        for j in groups[0]:
            settle(j)
    with scope("fwdz"):
        forward(rest[-1])
    with scope("arrive1"):
        for j in groups[1]:
            arrive(j)
    with scope("pre1"):
        expert_pre(1)
    with scope("back1"):
        back(1, 1)
        back(1, 0)
    with scope("part1"):
        expert_part(1, tp ^ 2)
        expert_part(1, tp)
    with scope("cross1"):
        for j in far_first(1):
            cross(j)
        for j in groups[1]:
            settle(j)
    with scope("home0"):
        for j in far_first(0):
            home(j)
    with scope("mix1"):
        mix_blocks(lambda m, i: m % 2 == 0)
    turns = list(range(8))

    def turn(count):
        for i in turns[:count]:
            wide = x_full // 8
            at = slice(i * wide, (i + 1) * wide)
            r.xt[at, :] = xr[:, at].T
        del turns[:count]

    for i, j in enumerate(far_first(1)):
        with scope("turn"):
            turn(2)
        with scope(f"home{steps[j]}"):
            home(j)
    with scope("turn"):
        turn(len(turns))
        r.act_t[...] = act[...].T
    mix_blocks(lambda m, i: m == 1)
    with scope("total"):
        total = r.cs[...].astype(f32)
        for g in range(2):
            for j in far_first(g):
                if steps[j]:
                    homes[j].wait_recv()
            total = total + jnp.dot(
                comb[:, groups[g][0] * cap : (groups[g][-1] + 1) * cap],
                ret[span(g), :],
                preferred_element_type=f32,
            )
        res[:, cols(tp)] = total.astype(bf16)
    with scope("tail"):
        tails = {}
        cut = tokens // 2

        def of(h, t):
            return res.at[pl.ds(h * cut, cut), cols(t)]

        for h in range(2):
            mine = of(h, tp)
            tails["across", h] = remote(mine, mine, tsems, 0, (h,), (sp, tp ^ 2))
            tails["across", h].start()
            tails["beside", h] = remote(mine, mine, tsems, 1, (h,), (sp, tp ^ 1))
            tails["beside", h].start()
        mix_blocks(lambda m, i: True)
        for h in range(2):
            tails["across", h].wait_recv()
            theirs = of(h, tp ^ 2)
            tails["onward", h] = remote(theirs, theirs, tsems, 2, (h,), (sp, tp ^ 1))
            tails["onward", h].start()
        for h in range(2):
            tails["beside", h].wait_recv()
        for h in range(2):
            tails["onward", h].wait_recv()
        loads[13].wait()

    share = tokens // parts
    piece = res.shape[1] // peers
    order = gather_order(peers)
    where_of = {k: m for m, k in enumerate(order)}
    moved = {}

    def tokens_of(t):
        return pl.ds(pl.multiple_of(t * share, share), share)

    def landing(k, t):
        at = where_of[k] * tokens + t * share
        return r.ares.at[pl.ds(pl.multiple_of(at, share), share)]

    if piece % 128:
        for i in range(peers):
            r.cut[i] = res[:, i * piece : (i + 1) * piece]

    def slice_for(s, t):
        if piece % 128:
            return r.cut.at[s, tokens_of(t)]
        return res.at[tokens_of(t), pl.ds(pl.multiple_of(s * piece, piece), piece)]

    def slice_out(k):
        if k:
            moved[0, k] = remote(
                slice_for(sp ^ k, tp), landing(k, tp), r.fsems, 0, (k,), (sp ^ k, tp)
            )
        else:
            moved[0, k] = pltpu.make_async_copy(slice_for(sp, tp), landing(0, tp), r.fsems.at[0, 0])
        moved[0, k].start()

    def slice_on(k):
        if k:
            moved[0, k].wait_recv()
        else:
            moved[0, k].wait()
        here = landing(k, tp)
        moved[1, k] = remote(here, here, r.fsems, 1, (k,), (sp, tp ^ 2))
        moved[1, k].start()
        moved[2, k] = remote(here, here, r.fsems, 2, (k,), (sp, tp ^ 1))
        moved[2, k].start()

    def slice_forward(k):
        moved[1, k].wait_recv()
        here = landing(k, tp ^ 2)
        moved[3, k] = remote(here, here, r.fsems, 3, (k,), (sp, tp ^ 1))
        moved[3, k].start()

    with scope("slices"):
        for k in steps:
            slice_out(k)
    with scope("gradmix"):
        r.gm[...] = jnp.dot(res[...], r.wo[...], preferred_element_type=f32).astype(bf16)
    scan = Scan(r, peers, sp, tp, head_dim, ready)
    with scope("totals"):
        scan.begin()
    units = [(n, p) for n in range(scan.blocks) for p in range(scan.pairs)]
    rounds = len(bits)
    events = [functools.partial(scan.advance, i) for i in range(rounds)]
    per = -(-len(units) // (rounds + 1))
    todo = [units[i : i + per] for i in range(0, len(units), per)]
    later = [list(range(max(peers // 2, 1))), list(range(max(peers // 2, 1), peers))]
    if rounds == 1:
        later = [later[0] + later[1]]
    later = later + [[]] * (rounds - len(later))
    for i in range(rounds):
        with scope(f"unit{i}"):
            for n, p in todo[i] if i < len(todo) else ():
                scan.unit(n, p)
        with scope(f"scan{i}"):
            events[i]()
        with scope(f"slice_on{i}"):
            for k in later[i]:
                slice_on(k)
            for k in later[i - 1] if i else ():
                slice_forward(k)
    with scope("unitz"):
        for some in todo[rounds:]:
            for n, p in some:
                scan.unit(n, p)
    with scope("finish"):
        scan.finish()
    with scope("slicez"):
        for k in later[-1] if rounds <= 2 else ():
            slice_forward(k)
        for k in steps:
            moved[2, k].wait_recv()
            moved[3, k].wait_recv()
    with scope("mixend"):
        for m in range(peers // 2):
            gathers[m, len(bits) - 1].wait_recv()
    with scope("gradout"):
        r.d_out[...] = contract_rows(r.ares[...], mixbuf[...])
    for group in (firsts, crossings, partners, forwards, backs, homes, gathers):
        for copy in group.values():
            copy.wait_send()
    for key, copy in moved.items():
        if key != (0, 0):
            copy.wait_send()
    for copy in tails.values():
        copy.wait_send()
    scan.close()


def lanes_of(head_dim):
    lane = lax.broadcasted_iota(jnp.int32, (1, 128), 1)
    return [(lane >= a * head_dim) & (lane < (a + 1) * head_dim) for a in range(128 // head_dim)]


def block_mask(head_dim):
    row = lax.broadcasted_iota(jnp.int32, (128, 128), 0)
    lane = lax.broadcasted_iota(jnp.int32, (128, 128), 1)
    mask = jnp.zeros((128, 128), jnp.float32)
    for a in range(128 // head_dim):
        low, high = a * head_dim, (a + 1) * head_dim
        inside = (row >= low) & (row < high) & (lane >= low) & (lane < high)
        mask = jnp.where(inside, 1.0, mask)
    return mask


def stacked(values, head_dim):
    keep = [jnp.where(m, 1.0, 0.0).astype(jnp.bfloat16) for m in lanes_of(head_dim)]
    return jnp.concatenate([values * m for m in keep], axis=0)


def retention_prepare(r, peers, sp, tp, head_dim):
    f32, bf16 = jnp.float32, jnp.bfloat16
    heads, tokens = r.logs_ref.shape
    pairs = r.q_ref.shape[1] // 128
    per = 128 // head_dim
    blocks = r.states_ref.shape[0] // (heads * head_dim)
    size = tokens // blocks
    picks = lanes_of(head_dim)
    row = lax.broadcasted_iota(jnp.int32, (size, size), 0)
    col = lax.broadcasted_iota(jnp.int32, (size, size), 1)
    upto = jnp.where(row <= col, 1.0, 0.0).astype(bf16)
    causal = row >= col
    logs = r.logs_ref[...]
    high = logs.astype(bf16).astype(f32)
    middle = (logs - high).astype(bf16).astype(f32)
    low = logs - high - middle
    split = jnp.concatenate([high, middle, low], axis=0).astype(bf16)
    spare = jnp.zeros((128 - heads, size), f32)

    def expand(values, p):
        out = values[:, p * per : p * per + 1]
        for a in range(1, per):
            out = jnp.where(picks[a], values[:, p * per + a : p * per + a + 1], out)
        return jnp.where(picks[0], values[:, p * per : p * per + 1], out)

    before = jnp.zeros((1, 128), f32)
    tile = jnp.zeros((head_dim, 128), f32)
    d_at = lax.broadcasted_iota(jnp.int32, (head_dim, 128), 0)
    l_at = lax.broadcasted_iota(jnp.int32, (head_dim, 128), 1)
    for a in range(per):
        tile = jnp.where(l_at == d_at + a * head_dim, 1.0, tile)
    tile = tile.astype(bf16)
    diagonal = block_mask(head_dim)
    for n in range(blocks):
        at = slice(n * size, (n + 1) * size)
        sums = jnp.dot(split[:, at], upto, preferred_element_type=f32)
        cum_t = sums[:heads] + sums[heads : 2 * heads] + sums[2 * heads :]
        cum = jnp.concatenate([cum_t, spare], axis=0).T
        end = cum[size - 1 : size, :]
        from_start = jnp.exp(cum)
        to_end = jnp.exp(end - cum)
        from_device = jnp.exp(cum + before)
        end_factor = jnp.exp(end)
        before = before + end
        for p in range(pairs):
            u = n * pairs + p
            lanes = slice(p * 128, (p + 1) * 128)
            q = r.q_ref[at, lanes]
            k = r.k_ref[at, lanes]
            begin = expand(from_start, p)
            r.fs[at, lanes] = begin
            r.te[at, lanes] = expand(to_end, p)
            r.rq[at, lanes] = (q.astype(f32) * begin).astype(bf16)
            r.tq[at, lanes] = (q.astype(f32) * expand(from_device, p)).astype(bf16)
            r.ends[n, p : p + 1, :] = expand(end_factor, p)
            for a in range(per):
                h = p * per + a
                gap = cum[:, h : h + 1] - cum_t[h : h + 1, :]
                r.dec[u, a * size : (a + 1) * size, :] = jnp.where(
                    causal, jnp.exp(jnp.minimum(gap, 0.0)), 0.0
                )
            score = contract_cols(stacked(q, head_dim), k)
            r.ws[u] = (score * r.dec[u]).astype(bf16)
            start = (n * heads + p * per) * head_dim
            states = r.states_ref[start : start + 128, :]
            wide = jnp.dot(states, tile, preferred_element_type=f32)
            r.stbd[u] = (wide * diagonal).astype(bf16)
    for p in range(pairs):
        r.own_log[p : p + 1, :] = expand(before, p)
    for p in range(pairs, 8):
        r.own_log[p : p + 1, :] = jnp.zeros((1, 128), f32)
    r.all_logs[sp] = r.own_log[...]
    copies = []
    for k in range(1, peers):
        copy = remote(r.own_log, r.all_logs.at[sp], r.gsems, 0, (k,), (sp ^ k, tp))
        copy.start()
        copies.append(copy)
    return copies


class Scan:
    def __init__(self, r, peers, sp, tp, head_dim, logs):
        self.r, self.peers, self.sp, self.tp, self.head_dim = r, peers, sp, tp, head_dim
        heads = r.logs_ref.shape[0]
        self.pairs = r.q_ref.shape[1] // 128
        self.per = 128 // head_dim
        self.blocks = r.states_ref.shape[0] // (heads * head_dim)
        self.size = r.logs_ref.shape[1] // self.blocks
        self.logs = logs
        self.sent = []

    def fold(self, full):
        full = full * block_mask(self.head_dim)
        out = full[: self.head_dim]
        for a in range(1, self.per):
            out = out + full[a * self.head_dim : (a + 1) * self.head_dim]
        return out

    def rows(self, p):
        return slice(p * self.head_dim, (p + 1) * self.head_dim)

    def second(self, n):
        start = (self.blocks + n) * self.size
        return slice(start, start + self.size)

    def begin(self):
        r = self.r
        for p in range(self.pairs):
            lanes = slice(p * 128, (p + 1) * 128)
            r.tot[self.rows(p), :] = self.fold(contract_rows(r.tq[:, lanes], r.gm[:, lanes]))
        r.suffix[...] = jnp.zeros(r.suffix.shape, jnp.float32)
        self.push(0)
        for copy in self.logs:
            copy.wait_recv()

    def push(self, i):
        r = self.r
        r.tsend[i] = r.tot[...].astype(jnp.bfloat16)
        copy = remote(
            r.tsend.at[i], r.trecv.at[i], r.ssems, 0, (i,), (self.sp ^ (1 << i), self.tp)
        )
        copy.start()
        self.sent.append(copy)

    def advance(self, i):
        r, sp, b = self.r, self.sp, 1 << i
        lower = (sp // b) % 2 == 0
        mine, base = sp // b, (sp // (2 * b)) * 2
        reach = jnp.zeros((8, 128), jnp.float32)
        group = jnp.zeros((8, 128), jnp.float32)
        for m in range(self.peers):
            ahead = jnp.where(jnp.logical_and(sp < m, mine == m // b), 1.0, 0.0)
            reach = reach + ahead * r.all_logs[m]
            group = group + jnp.where(base == m // b, 1.0, 0.0) * r.all_logs[m]
        up = jnp.where(lower, 1.0, 0.0)
        reach = jnp.exp(reach) * up
        group = jnp.exp(group)
        self.sent[i].wait_recv()
        for p in range(self.pairs):
            at = self.rows(p)
            mine_t = r.tot[at, :]
            theirs = r.trecv[i, at, :].astype(jnp.float32)
            r.suffix[at, :] = r.suffix[at, :] + reach[p : p + 1, :] * theirs
            early = up * mine_t + (1.0 - up) * theirs
            late = up * theirs + (1.0 - up) * mine_t
            r.tot[at, :] = early + group[p : p + 1, :] * late
        if 2 * b < self.peers:
            self.push(i + 1)

    def unit(self, n, p):
        r, size = self.r, self.size
        f32, bf16 = jnp.float32, jnp.bfloat16
        at = slice(n * size, (n + 1) * size)
        lanes = slice(p * 128, (p + 1) * 128)
        u = n * self.pairs + p
        g, v, k, q = r.gm[at, lanes], r.v_ref[at, lanes], r.k_ref[at, lanes], r.q_ref[at, lanes]
        grads = stacked(g, self.head_dim)
        weighted = (contract_cols(grads, v) * r.dec[u]).astype(bf16)
        wide = jnp.concatenate(
            [weighted[a * size : (a + 1) * size] for a in range(self.per)], axis=1
        )
        intra = jnp.dot(wide, stacked(k, self.head_dim), preferred_element_type=f32)
        carry = contract_cols(g, r.stbd[u])
        r.gq[at, lanes] = (intra + carry * r.fs[at, lanes]).astype(bf16)
        r.acc[at, lanes] = contract_rows(weighted, stacked(q, self.head_dim))
        r.acc[self.second(n), lanes] = contract_rows(r.ws[u], grads)
        r.outer[n, self.rows(p), :] = self.fold(contract_rows(r.rq[at, lanes], g))

    def finish(self):
        r, size = self.r, self.size
        bf16 = jnp.bfloat16
        diagonal = block_mask(self.head_dim)
        for p in range(self.pairs):
            lanes = slice(p * 128, (p + 1) * 128)
            state = r.suffix[self.rows(p), :]
            for n in reversed(range(self.blocks)):
                at = slice(n * size, (n + 1) * size)
                rounded = state.astype(bf16).astype(jnp.float32)
                full = (jnp.concatenate([rounded] * self.per, axis=0) * diagonal).astype(bf16)
                v, k = r.v_ref[at, lanes], r.k_ref[at, lanes]
                te = r.te[at, lanes]
                r.gk[at, lanes] = (r.acc[at, lanes] + contract_cols(v, full) * te).astype(bf16)
                r.gv[at, lanes] = (
                    r.acc[self.second(n), lanes]
                    + jnp.dot(k, full, preferred_element_type=jnp.float32) * te
                ).astype(bf16)
                if n:
                    state = r.ends[n, p : p + 1, :] * state + r.outer[n, self.rows(p), :]

    def close(self):
        for copy in self.logs + self.sent:
            copy.wait_send()


def layer_backward(arrays, peers, parts, capacity, head_dim):
    cap = -(-capacity // 16) * 16
    tokens, full = arrays["x_hbm"].shape
    hidden = arrays["gate_hbm"].shape[1]
    local = arrays["q_hbm"].shape[1]
    blocks = arrays["states_hbm"].shape[0] // local
    size = tokens // blocks
    pairs = local // 128
    units = blocks * pairs
    width = full // parts
    piece = full // peers
    total = peers * cap
    most = max(len(g) for g in peer_groups(peers)) * cap
    bits = peers.bit_length() - 1
    bf16, f32 = jnp.bfloat16, jnp.float32

    def shape(*dims, dtype=bf16):
        return jax.ShapeDtypeStruct(dims, dtype)

    def vmem(*dims, dtype=bf16):
        return pltpu.VMEM(dims, dtype)

    outs = dict(
        xt=shape(full, total),
        gr=shape(total, full),
        act_t=shape(hidden, total),
        gg=shape(total, hidden),
        ug=shape(total, hidden),
        d_out=shape(piece, local, dtype=f32),
        gq=shape(tokens, local),
        gk=shape(tokens, local),
        gv=shape(tokens, local),
    )
    scratch = dict(
        ares=vmem(peers * tokens, piece),
        mixbuf=vmem(peers * tokens, local),
        xs=vmem(tokens, width),
        cs=vmem(tokens, width),
        q_ref=vmem(tokens, local),
        k_ref=vmem(tokens, local),
        v_ref=vmem(tokens, local),
        routes_ref=vmem(*arrays["routes_hbm"].shape, dtype=jnp.int32),
        weights_ref=vmem(*arrays["weights_hbm"].shape, dtype=f32),
        logs_ref=vmem(*arrays["logs_hbm"].shape, dtype=f32),
        states_ref=vmem(*arrays["states_hbm"].shape),
        wg=vmem(full, hidden),
        wu=vmem(full, hidden),
        wd=vmem(hidden, full),
        wo=vmem(full, local),
        xr=vmem(total, full),
        sx=vmem(total, width),
        sg=vmem(total, width),
        pre_g=vmem(most, hidden, dtype=f32),
        pre_u=vmem(most, hidden, dtype=f32),
        act=vmem(total, hidden),
        part=vmem(total, full),
        rx1=vmem(2, total, width),
        acc=vmem(total, width, dtype=f32),
        sb=vmem(total, width),
        rx2=vmem(total, width),
        ret=vmem(total, width),
        comb=vmem(tokens, total),
        res=vmem(tokens, full),
        gm=vmem(tokens, local),
        rq=vmem(tokens, local),
        tq=vmem(tokens, local),
        fs=vmem(tokens, local, dtype=f32),
        te=vmem(tokens, local, dtype=f32),
        dec=vmem(units, 128 // head_dim * size, size, dtype=f32),
        ws=vmem(units, 128 // head_dim * size, size),
        stbd=vmem(units, 128, 128),
        ends=vmem(blocks, 8, 128, dtype=f32),
        own_log=vmem(8, 128, dtype=f32),
        all_logs=vmem(peers, 8, 128, dtype=f32),
        tot=vmem(pairs * head_dim, 128, dtype=f32),
        suffix=vmem(pairs * head_dim, 128, dtype=f32),
        outer=vmem(blocks, pairs * head_dim, 128, dtype=f32),
        tsend=vmem(bits, pairs * head_dim, 128),
        trecv=vmem(bits, pairs * head_dim, 128),
        dsems=pltpu.SemaphoreType.DMA((8, 2, peers)),
        rsems=pltpu.SemaphoreType.DMA((8, peers)),
        tsems=pltpu.SemaphoreType.DMA((6, 2)),
        msems=pltpu.SemaphoreType.DMA((2, peers)),
        lsems=pltpu.SemaphoreType.DMA((14,)),
        fsems=pltpu.SemaphoreType.DMA((8, peers)),
        gsems=pltpu.SemaphoreType.DMA((2, peers)),
        ssems=pltpu.SemaphoreType.DMA((2, bits)),
    )
    if piece % 128:
        scratch["cut"] = vmem(peers, tokens, piece)
    names = list(arrays) + list(outs) + list(scratch)

    def place(name, value):
        if name.endswith("hbm"):
            return pltpu.with_memory_space_constraint(value, pltpu.HBM)
        return value

    results = pl.pallas_call(
        functools.partial(layer_kernel, peers, parts, cap, head_dim, names),
        out_shape=tuple(outs.values()),
        in_specs=[HBM if name.endswith("hbm") else VMEM for name in arrays],
        out_specs=(VMEM,) * len(outs),
        scratch_shapes=list(scratch.values()),
        compiler_params=pltpu.CompilerParams(
            collective_id=0, has_side_effects=True, vmem_limit_bytes=(42 if peers <= 8 else 63) * 2**20
        ),
        name="layer_backward",
    )(*[place(name, value) for name, value in arrays.items()])
    return weight_grads(*results)


def weights_kernel(
    xt, g, act, gg, ug, i_out, i_q, i_k, i_v,
    d_gate, d_up, d_down, d_out, o_q, o_k, o_v,
    v_gate, v_up, v_down, osems,
):
    full = v_gate.shape[0]
    count, parts = 8, 4
    wide, broad = full // count, full // parts
    f32 = jnp.float32
    stores = []

    def store(src, dst):
        copy = pltpu.make_async_copy(src, dst, osems.at[len(stores)])
        copy.start()
        stores.append(copy)

    for i in range(count):
        at = slice(i * wide, (i + 1) * wide)
        v_gate[at, :] = jnp.dot(xt[at, :], gg[...], preferred_element_type=f32)
        store(v_gate.at[at], d_gate.at[at])
        v_up[at, :] = jnp.dot(xt[at, :], ug[...], preferred_element_type=f32)
        store(v_up.at[at], d_up.at[at])
    for src, dst in ((i_out, d_out), (i_q, o_q), (i_k, o_k), (i_v, o_v)):
        store(src, dst)
    for i in range(parts):
        at = slice(i * broad, (i + 1) * broad)
        v_down[:, at] = jnp.dot(act[...], g[:, at], preferred_element_type=f32)
        store(v_down.at[:, at], d_down.at[:, at])
    for copy in stores:
        copy.wait()


def weight_grads(xt, g, act, gg, ug, d_out, q, k, v):
    full, total = xt.shape
    hidden = act.shape[0]
    f32 = jnp.float32
    grads = [jax.ShapeDtypeStruct(s, f32) for s in ((full, hidden), (full, hidden), (hidden, full))]
    others = [jax.ShapeDtypeStruct(a.shape, a.dtype) for a in (d_out, q, k, v)]
    limit = 62 if total > 640 else 20
    return pl.pallas_call(
        weights_kernel,
        out_shape=tuple(grads + others),
        in_specs=[VMEM] * 9,
        out_specs=(HBM,) * 7,
        scratch_shapes=[pltpu.VMEM(a.shape, a.dtype) for a in grads]
        + [pltpu.SemaphoreType.DMA((24,))],
        compiler_params=pltpu.CompilerParams(vmem_limit_bytes=limit * 2**20),
        name="weight_grads",
    )(xt, g, act, gg, ug, d_out, q, k, v)


def shards(
    moe_input,
    cotangent,
    routes,
    route_weights,
    gate_weight,
    up_weight,
    down_weight,
    out_weight,
    mixer_output,
    queries,
    key_vectors,
    value_vectors,
    log_decay,
    block_states,
):
    tok_dev, model_width = cotangent.shape
    peers, parts = lax.axis_size("sp"), lax.axis_size("tp")
    capacity = 5 * tok_dev * TOP_K // (4 * peers)
    head_dim = block_states.shape[-1]
    arrays = dict(
        routes_hbm=routes.T,
        weights_hbm=route_weights.T,
        x_hbm=moe_input,
        cot_hbm=cotangent,
        gate_hbm=gate_weight[0],
        up_hbm=up_weight[0],
        down_hbm=down_weight[0],
        out_hbm=out_weight,
        mix_hbm=mixer_output,
        q_hbm=queries,
        k_hbm=key_vectors,
        v_hbm=value_vectors,
        logs_hbm=log_decay.T,
        states_hbm=block_states.reshape(-1, head_dim),
    )
    grad_gate, grad_up, grad_down, *others = layer_backward(
        arrays, peers, parts, capacity, head_dim
    )
    return (grad_gate[None], grad_up[None], grad_down[None], *others)


def solution(mesh):
    return jax.shard_map(
        shards,
        mesh=mesh,
        in_specs=(
            P("sp", None),
            P("sp", None),
            P("sp", None),
            P("sp", None),
            P("sp", None, "tp"),
            P("sp", None, "tp"),
            P("sp", "tp", None),
            P(None, "tp"),
            P("sp", "tp"),
            P("sp", "tp"),
            P("sp", "tp"),
            P("sp", "tp"),
            P("sp", "tp"),
            P("sp", "tp", None, None),
        ),
        out_specs=(
            P("sp", None, "tp"),
            P("sp", None, "tp"),
            P("sp", "tp", None),
            P("sp", "tp"),
            P("sp", "tp"),
            P("sp", "tp"),
            P("sp", "tp"),
        ),
        check_vma=False,
    )
```
